32 devices in a mesh: sp: 8 (over z, y), tp: 4 (over x, core).
Axes of the slice: x: 2, y: 2, z: 4, core: 2. Of those that a mesh axis runs over, the one named last changes fastest.
Arguments:
- mixer_value_projection: bfloat16 [6144, 2048], P('sp', 'tp'), may hold values from -6 to 6
- write_vectors_projected: bfloat16 [6144, 256], P('sp', 'tp'), may hold values from -6 to 6
- read_vectors_projected: bfloat16 [6144, 256], P('sp', 'tp'), may hold values from -6 to 6
- output_gate_projected: bfloat16 [6144, 2048], P('sp', 'tp'), may hold values from -6 to 6
- step_size_scores: float32 [6144, 32], P('sp', 'tp'), may hold values from -8 to 8
- position_decay_extra: float32 [6144, 32], P('sp', 'tp'), may hold values from -1 to 0
- step_size_bias: float32 [32], P('tp'), may hold values from -1 to 1
- head_decay_logarithm: float32 [32], P('tp'), may hold values from -14 to -3
- value_filter_taps: bfloat16 [4, 2048], P(None, 'tp'), may hold values from -3 to 3
- write_filter_taps: bfloat16 [4, 256], P(None, 'tp'), may hold values from -3 to 3
- read_filter_taps: bfloat16 [4, 256], P(None, 'tp'), may hold values from -3 to 3
- gated_group_norm_gain: float32 [2048], P('tp'), may hold values from 0.1 to 1.9
- mixer_output_weight: bfloat16 [2048, 2048], P('tp'), may hold values from -0.125 to 0.125
- residual: bfloat16 [6144, 2048], P('sp'), may hold values from -6 to 6
- feedforward_norm_gain: float32 [2048], replicated, may hold values from 0.1 to 1.9
- feedforward_gate_weight: bfloat16 [2048, 5632], P('sp', 'tp'), may hold values from -0.125 to 0.125
- feedforward_value_weight: bfloat16 [2048, 5632], P('sp', 'tp'), may hold values from -0.125 to 0.125
- gate_filter_taps: bfloat16 [3, 5632], P(None, 'tp'), may hold values from -3.5 to 3.5
- single_value_filter_taps: bfloat16 [3, 5632], P(None, 'tp'), may hold values from -3.5 to 3.5
- feedforward_down_weight: bfloat16 [5632, 2048], P('tp', 'sp'), may hold values from -0.078125 to 0.078125
Outputs:
- mixed: bfloat16 [6144, 2048], P(('sp', 'tp'))
The draws below stay inside these ranges and needn't reach their ends.
All inputs are finite; a program needn't handle non-finite values.
Results may differ from the reference program's by a relative error of at most 0.012.
Values may be sent and summed in bfloat16 or wider, within the bound.
A program may use at most 192 MiB of HBM per device.

```python
import jax
import jax.numpy as jnp
from jax import lax

D = 2048
HEADS = 32
HEAD = 64
GROUPS = 4
STATE = 64
FF = 5632
TOK_DEV = 768
BLOCK = 128
CONV_MIX = 4
CONV_FFN = 3
INNER = 2048
SEQ = 6144


def draw_step_size_scores(key, part):
    first, second = jax.random.split(jax.random.fold_in(key, 11))
    block_total = SEQ // TOK_DEV
    base = jax.random.normal(first, (SEQ, HEADS), jnp.float32)
    shifts = jax.random.uniform(second, (block_total, 1, HEADS), jnp.float32, -1.5, 1.5)
    return (base.reshape(block_total, TOK_DEV, HEADS) + shifts).reshape(SEQ, HEADS)


def draw_head_decay_logarithm(key, part):
    first, second, third = jax.random.split(jax.random.fold_in(key, 12), 3)
    share = 0.5
    slowly = jax.random.uniform(first, (HEADS,), jnp.float32) < share
    slow_rate = jnp.log(jax.random.uniform(second, (HEADS,), jnp.float32, 0.4, 1.0) / SEQ)
    fast_rate = jax.random.uniform(third, (HEADS,), jnp.float32, jnp.log(1.0 / 60.0), jnp.log(1.0 / 25.0))
    return jnp.where(slowly, slow_rate, fast_rate)


def draw_position_decay_extra(key, part):
    first, second = jax.random.split(jax.random.fold_in(key, 13))
    places = jax.random.randint(first, (3,), 0, SEQ)
    losses = jnp.log(jax.random.uniform(second, (3, HEADS), jnp.float32, 0.5, 0.8))
    positions = jnp.arange(SEQ)
    hits = (positions[:, None] == places[None, :]).astype(jnp.float32)
    return jnp.sum(hits[:, :, None] * losses[None, :, :], axis=1)


def block_levels(rng, dims, cuts, smallest, top_value):
    level = 1.0
    for position, parts in cuts:
        heights = jax.random.uniform(jax.random.fold_in(jax.random.fold_in(rng, 6), position), (parts,), jnp.float32, smallest / len(cuts), top_value / len(cuts))
        level = level * jnp.repeat(jnp.exp(heights), dims[position] // parts).reshape((-1,) + (1,) * (len(dims) - 1 - position))
    return level


def scatter_about(own_key, extent, deviation, bound, pieces=(), held_as=jnp.bfloat16):
    loudness = block_levels(own_key, extent, pieces, -0.22, 0.18) if pieces else 1.0
    array = jax.random.normal(own_key, extent, jnp.float32) * deviation * loudness
    return jnp.minimum(jnp.maximum(array, -bound), bound).astype(held_as)


def setup_inputs(seed: int = 0) -> dict:
    streams_of = jax.random.split(jax.random.key(seed), 21)
    mixer_value_projection = scatter_about(streams_of[0], (SEQ, INNER), 1.0, 6.0, ((0, 8), (1, 4)))
    write_vectors_projected = scatter_about(streams_of[1], (SEQ, GROUPS * STATE), 1.0, 6.0, ((0, 8), (1, 4)))
    read_vectors_projected = scatter_about(streams_of[2], (SEQ, GROUPS * STATE), 1.0, 6.0, ((0, 8), (1, 4)))
    output_gate_projected = scatter_about(streams_of[3], (SEQ, INNER), 1.0, 6.0, ((0, 8), (1, 4)))
    step_size_scores = draw_step_size_scores(jax.random.fold_in(streams_of[20], 71), 0)
    position_decay_extra = draw_position_decay_extra(jax.random.fold_in(streams_of[20], 71), 0)
    step_size_bias = jnp.clip(jax.random.uniform(streams_of[6], (HEADS,), jnp.float32, -1.0, 1.0) * block_levels(streams_of[6], (HEADS,), ((0, 4),), -0.4, 0.0), -1.0, 1.0)
    head_decay_logarithm = draw_head_decay_logarithm(jax.random.fold_in(streams_of[20], 71), 0)
    value_filter_taps = scatter_about(streams_of[8], (CONV_MIX, INNER), CONV_MIX ** -0.5, 3.0, ((1, 4),))
    write_filter_taps = scatter_about(streams_of[9], (CONV_MIX, GROUPS * STATE), CONV_MIX ** -0.5, 3.0, ((1, 4),))
    read_filter_taps = scatter_about(streams_of[10], (CONV_MIX, GROUPS * STATE), CONV_MIX ** -0.5, 3.0, ((1, 4),))
    gated_group_norm_gain = jnp.clip(1.0 + 0.18 * jax.random.normal(streams_of[11], (INNER,), jnp.float32), 0.1, 1.9)
    mixer_output_weight = scatter_about(streams_of[12], (INNER, D), INNER ** -0.5, 0.125, ((0, 4),))
    residual = scatter_about(streams_of[13], (SEQ, D), 1.0, 6.0, ((0, 8),))
    feedforward_norm_gain = jnp.clip(1.0 + 0.18 * jax.random.normal(streams_of[14], (D,), jnp.float32), 0.1, 1.9)
    feedforward_gate_weight = scatter_about(streams_of[15], (D, FF), D ** -0.5, 0.125, ((0, 8), (1, 4)))
    feedforward_value_weight = scatter_about(streams_of[16], (D, FF), D ** -0.5, 0.125, ((0, 8), (1, 4)))
    gate_filter_taps = scatter_about(streams_of[17], (CONV_FFN, FF), CONV_FFN ** -0.5, 3.5, ((1, 4),))
    single_value_filter_taps = scatter_about(streams_of[18], (CONV_FFN, FF), CONV_FFN ** -0.5, 3.5, ((1, 4),))
    feedforward_down_weight = scatter_about(streams_of[19], (FF, D), FF ** -0.5, 0.078125, ((0, 4), (1, 8)))
    return {"mixer_value_projection": mixer_value_projection, "write_vectors_projected": write_vectors_projected, "read_vectors_projected": read_vectors_projected, "output_gate_projected": output_gate_projected, "step_size_scores": step_size_scores, "position_decay_extra": position_decay_extra, "step_size_bias": step_size_bias, "head_decay_logarithm": head_decay_logarithm, "value_filter_taps": value_filter_taps, "write_filter_taps": write_filter_taps, "read_filter_taps": read_filter_taps, "gated_group_norm_gain": gated_group_norm_gain, "mixer_output_weight": mixer_output_weight, "residual": residual, "feedforward_norm_gain": feedforward_norm_gain, "feedforward_gate_weight": feedforward_gate_weight, "feedforward_value_weight": feedforward_value_weight, "gate_filter_taps": gate_filter_taps, "single_value_filter_taps": single_value_filter_taps, "feedforward_down_weight": feedforward_down_weight}


epsilon = 1e-06

def causal_taps(current, kernel):
    tap_count = kernel.shape[0]
    length = current.shape[0]
    padded = jnp.concatenate([jnp.zeros((tap_count - 1, current.shape[1]), current.dtype), current], 0).astype(jnp.float32)
    result = jnp.zeros((length, current.shape[1]), jnp.float32)
    for offset in range(tap_count):
        result = result + kernel[offset].astype(jnp.float32) * padded[offset:offset + length]
    return result

def channel_norm(stream, gain):
    floats = stream.astype(jnp.float32)
    scaled = floats * lax.rsqrt(lax.optimization_barrier(jnp.mean(floats * floats, axis=-1, keepdims=True)) + epsilon)
    return (scaled * gain).astype(jnp.bfloat16)

def reference(mixer_value_projection, write_vectors_projected, read_vectors_projected, output_gate_projected, step_size_scores, position_decay_extra, step_size_bias, head_decay_logarithm, value_filter_taps, write_filter_taps, read_filter_taps, gated_group_norm_gain, mixer_output_weight, residual, feedforward_norm_gain, feedforward_gate_weight, feedforward_value_weight, gate_filter_taps, single_value_filter_taps, feedforward_down_weight):
    per_group = HEADS // GROUPS
    x_conv = jax.nn.silu(causal_taps(mixer_value_projection, value_filter_taps)).astype(jnp.bfloat16)
    write_conv = jax.nn.silu(causal_taps(write_vectors_projected, write_filter_taps)).astype(jnp.bfloat16)
    read_conv = jax.nn.silu(causal_taps(read_vectors_projected, read_filter_taps)).astype(jnp.bfloat16)
    step_size_head = jax.nn.softplus(step_size_scores + step_size_bias)
    logarithm_decay_rate = -step_size_head * jnp.exp(head_decay_logarithm) + position_decay_extra
    scaled = (x_conv.astype(jnp.float32).reshape(SEQ, HEADS, HEAD) * step_size_head[:, :, None]).astype(jnp.bfloat16)
    block_count = SEQ // BLOCK
    value_blocks = scaled.reshape(block_count, BLOCK, GROUPS, per_group, HEAD)
    write_blocks = write_conv.reshape(block_count, BLOCK, GROUPS, STATE)
    read_blocks = read_conv.reshape(block_count, BLOCK, GROUPS, STATE)
    log_blocks = logarithm_decay_rate.reshape(block_count, BLOCK, HEADS)
    causal = jnp.tril(jnp.ones((BLOCK, BLOCK), dtype=jnp.bool_))

    def block_step(carried, inputs):
        value_rows, write_rows, read_rows, log_rows = inputs
        running = jnp.cumsum(log_rows, axis=0)
        by_head = running.T
        spread = by_head[:, :, None] - by_head[:, None, :]
        decays = jnp.exp(jnp.where(causal, spread, -jnp.inf)).reshape(GROUPS, per_group, BLOCK, BLOCK)
        scores = jnp.einsum('lgn,sgn->gls', read_rows.astype(jnp.float32), write_rows.astype(jnp.float32))
        weights = (scores[:, None] * decays).astype(jnp.bfloat16)
        inside = jnp.einsum('grls,sgrp->lgrp', weights.astype(jnp.float32), value_rows.astype(jnp.float32))
        entering = jnp.einsum('lgn,grnp->lgrp', read_rows.astype(jnp.float32), carried, precision=lax.Precision.HIGHEST)
        entering = entering * jnp.exp(running).reshape(BLOCK, GROUPS, per_group)[..., None]
        tails = jnp.exp(by_head[:, -1:] - by_head).T.reshape(BLOCK, GROUPS, per_group)
        tailed = (value_rows.astype(jnp.float32) * tails[..., None]).astype(jnp.bfloat16)
        fresh = jnp.einsum('sgn,sgrp->grnp', write_rows.astype(jnp.float32), tailed.astype(jnp.float32))
        advanced = carried * jnp.exp(running[-1]).reshape(GROUPS, per_group)[..., None, None] + fresh
        return (advanced, inside + entering)
    start_state = jnp.zeros((GROUPS, per_group, STATE, HEAD), jnp.float32)
    outputs = lax.scan(block_step, start_state, (value_blocks, write_blocks, read_blocks, log_blocks))[1]
    mixer = outputs.reshape(SEQ, INNER)
    gated = (mixer * jax.nn.silu(output_gate_projected.astype(jnp.float32))).reshape(SEQ, GROUPS, INNER // GROUPS)
    gated = gated * lax.rsqrt(lax.optimization_barrier(jnp.mean(gated * gated, axis=-1, keepdims=True)) + epsilon)
    normed = (gated.reshape(SEQ, INNER) * gated_group_norm_gain).astype(jnp.bfloat16)
    stream = (residual.astype(jnp.float32) + jnp.dot(normed, mixer_output_weight, preferred_element_type=jnp.float32)).astype(jnp.bfloat16)
    ffn_in = channel_norm(stream, feedforward_norm_gain)
    gate_rows = jnp.dot(ffn_in, feedforward_gate_weight, preferred_element_type=jnp.float32).astype(jnp.bfloat16)
    value_rows = jnp.dot(ffn_in, feedforward_value_weight, preferred_element_type=jnp.float32).astype(jnp.bfloat16)
    hidden = (jax.nn.silu(causal_taps(gate_rows, gate_filter_taps)) * causal_taps(value_rows, single_value_filter_taps)).astype(jnp.bfloat16)
    down = jnp.dot(hidden, feedforward_down_weight, preferred_element_type=jnp.float32)
    return (stream.astype(jnp.float32) + down).astype(jnp.bfloat16)
```

```python
import functools

import jax
import jax.numpy as jnp
from jax import lax
from jax.experimental import pallas as pl
from jax.experimental.pallas import tpu as pltpu
from jax.sharding import PartitionSpec as P

HEAD = 64
STATE = 64
BLOCK = 128


epsilon = 1e-06


def from_behind(value, axis, by):
    length = lax.axis_size(axis)
    pairs = [(i, i + by) for i in range(length) if 0 <= i + by < length]
    return lax.ppermute(value, axis, pairs)


def entering_2(value, axis, join, neutral):
    count, mine = (lax.axis_size(axis), lax.axis_index(axis))

    def shifted(part, by):
        moved = from_behind(part, axis, by)
        return jnp.where(mine >= by, moved, neutral)

    if count == 1:
        return neutral
    window, width = (shifted(value, 1), 1)
    while width < count - 1:
        earlier = shifted(value, 2) if width == 1 else shifted(window, width)
        window, width = (join(earlier, window), 2 * width)
    return window


def halving_bits(axis):
    count = lax.axis_size(axis)
    return [1 << b for b in range(count.bit_length() - 1)] if count & (count - 1) == 0 else None


def swap(value, axis, bit):
    return lax.ppermute(value, axis, [(i, i ^ bit) for i in range(lax.axis_size(axis))])


def product_scattered(rows, weight, axis):
    count, mine = (lax.axis_size(axis), lax.axis_index(axis))
    bits = halving_bits(axis)
    if not bits:
        product = jnp.dot(rows, weight, preferred_element_type=jnp.float32)
        return lax.psum_scatter(product, axis, scatter_dimension=0, tiled=True)
    share = rows.shape[0] // count

    def side(array, which):
        return lax.dynamic_index_in_dim(
            array.reshape(array.shape[0] // 2, 2, *array.shape[1:]),
            which,
            1,
            keepdims=False,
            allow_negative_indices=False,
        )

    rows = rows.reshape(count, share, -1)

    def multiplied(part):
        flat = jnp.dot(
            part.reshape(-1, part.shape[-1]), weight, preferred_element_type=jnp.float32
        )
        return flat.reshape(part.shape[0], share, -1)

    low = mine & 1
    product = multiplied(rows)
    going = side(product, 1 - low).astype(jnp.bfloat16)
    arrived = swap(going, axis, 1)
    total = side(product, low)
    for bit in bits[1:]:
        own = (mine // bit) & 1
        going = (side(total, 1 - own) + side(arrived, 1 - own).astype(jnp.float32)).astype(
            jnp.bfloat16
        )
        total = side(total, own) + side(arrived, own).astype(jnp.float32)
        arrived = swap(going, axis, bit)
    return (total + arrived.astype(jnp.float32))[0]


def rows_gathered(own, axis):
    bits = halving_bits(axis)
    if not bits:
        return lax.all_gather(own, axis, axis=0, tiled=True)
    mine = lax.axis_index(axis)
    held = own[None]
    for bit in reversed(bits):
        other = swap(held, axis, bit)
        high = ((mine // bit) & 1) == 1
        held = jnp.stack([jnp.where(high, other, held), jnp.where(high, held, other)], 1)
        held = held.reshape(-1, *own.shape)
    return held.reshape(-1, own.shape[-1])


def put(whole, block, index):
    start = (index, *[jnp.zeros_like(index)] * block.ndim)
    return lax.dynamic_update_slice(whole, block[None], start, allow_negative_indices=False)


class RingGather:
    def __init__(self, block, axis):
        self.axis, self.count, self.step = (axis, lax.axis_size(axis), 0)
        count, mine = (self.count, lax.axis_index(axis))
        if count % 2:
            order = list(range(count))
            self.place = mine
        else:
            order = list(range(0, count, 2)) + list(range(count - 1, 0, -2))
            self.place = jnp.where(mine % 2 == 0, mine, 2 * count - 1 - mine) // 2
        self.forward = [(order[p], order[(p + 1) % count]) for p in range(count)]
        self.backward = [(b, a) for a, b in self.forward]
        self.up = self.down = block
        whole = jnp.zeros((count, *block.shape), block.dtype)
        self.whole = put(whole, block, mine)

    def owner(self, place):
        place = lax.rem(place + self.count, self.count)
        if self.count % 2:
            return place
        return jnp.where(2 * place < self.count, 2 * place, 2 * self.count - 1 - 2 * place)

    def advance(self):
        self.step += 1
        if self.step > self.count // 2:
            return
        self.up = lax.ppermute(self.up, self.axis, self.forward)
        self.whole = put(self.whole, self.up, self.owner(self.place - self.step))
        if self.step <= (self.count - 1) // 2:
            self.down = lax.ppermute(self.down, self.axis, self.backward)
            self.whole = put(self.whole, self.down, self.owner(self.place + self.step))

    def settle(self, value):
        value, self.up, self.down = lax.optimization_barrier((value, self.up, self.down))
        return value

    def gathered(self):
        while self.step < self.count // 2:
            self.advance()
        return self.whole.reshape(-1, self.whole.shape[-1])


def causal_taps(current, previous, kernel):
    tap_count = kernel.shape[0]
    length = current.shape[0]
    padded = jnp.concatenate([previous, current], 0).astype(jnp.float32)
    result = jnp.zeros((length, current.shape[1]), jnp.float32)
    for offset in range(tap_count):
        result = result + kernel[offset].astype(jnp.float32) * padded[offset : offset + length]
    return result


def channel_norm(stream, gain):
    floats = stream.astype(jnp.float32)
    scaled = floats * lax.rsqrt(jnp.mean(floats * floats, axis=-1, keepdims=True) + epsilon)
    return (scaled * gain).astype(jnp.bfloat16)


def plain_on_device(
    mixer_value_projection,
    write_vectors_projected,
    read_vectors_projected,
    output_gate_projected,
    step_size_scores,
    position_decay_extra,
    step_size_bias,
    head_decay_logarithm,
    value_filter_taps,
    write_filter_taps,
    read_filter_taps,
    gated_group_norm_gain,
    mixer_output_weight,
    residual,
    feedforward_norm_gain,
    feedforward_gate_weight,
    feedforward_value_weight,
    gate_filter_taps,
    single_value_filter_taps,
    feedforward_down_weight,
):
    row_count = mixer_value_projection.shape[0]
    head_count = step_size_scores.shape[1]
    group_count = write_vectors_projected.shape[1] // STATE
    per_group = head_count // group_count
    mix_rim = value_filter_taps.shape[0] - 1
    channels = (mixer_value_projection.shape[1], write_vectors_projected.shape[1])
    rims = from_behind(
        jnp.concatenate(
            [
                mixer_value_projection[row_count - mix_rim :],
                write_vectors_projected[row_count - mix_rim :],
                read_vectors_projected[row_count - mix_rim :],
            ],
            1,
        ),
        "sp",
        1,
    )
    rim_values, rim_write, rim_read = jnp.split(rims, [channels[0], sum(channels)], axis=1)
    by_ring = feedforward_gate_weight.shape[1] // 256 * 128
    gate_ring = RingGather(feedforward_gate_weight[:, :by_ring], "sp")
    gate_ring.advance()
    x_conv = jax.nn.silu(causal_taps(mixer_value_projection, rim_values, value_filter_taps)).astype(
        jnp.bfloat16
    )
    write_conv = jax.nn.silu(
        causal_taps(write_vectors_projected, rim_write, write_filter_taps)
    ).astype(jnp.bfloat16)
    read_conv = jax.nn.silu(causal_taps(read_vectors_projected, rim_read, read_filter_taps)).astype(
        jnp.bfloat16
    )
    step_size_head = jax.nn.softplus(step_size_scores + step_size_bias)
    logarithm_decay_rate = -step_size_head * jnp.exp(head_decay_logarithm) + position_decay_extra
    scaled = (
        x_conv.astype(jnp.float32).reshape(row_count, head_count, HEAD) * step_size_head[:, :, None]
    ).astype(jnp.bfloat16)
    block_count = row_count // BLOCK
    value_blocks = scaled.reshape(block_count, BLOCK, group_count, per_group, HEAD)
    write_blocks = write_conv.reshape(block_count, BLOCK, group_count, STATE)
    read_blocks = read_conv.reshape(block_count, BLOCK, group_count, STATE)
    running = jnp.cumsum(logarithm_decay_rate.reshape(block_count, BLOCK, head_count), axis=1)
    by_head = jnp.moveaxis(running, 1, 2)
    spread = by_head[..., :, None] - by_head[..., None, :]
    causal = jnp.tril(jnp.ones((BLOCK, BLOCK), dtype=jnp.bool_))
    decays = jnp.exp(jnp.where(causal, spread, -jnp.inf)).reshape(
        block_count, group_count, per_group, BLOCK, BLOCK
    )
    scores = jnp.einsum(
        "blgn,bsgn->bgls", read_blocks, write_blocks, preferred_element_type=jnp.float32
    )
    weights = (scores[:, :, None] * decays).astype(jnp.bfloat16)
    inside = jnp.einsum(
        "bgrls,bsgrp->blgrp", weights, value_blocks, preferred_element_type=jnp.float32
    )
    tails = jnp.moveaxis(jnp.exp(by_head[..., -1:] - by_head), 2, 1).reshape(
        block_count, BLOCK, group_count, per_group
    )
    tailed = (value_blocks.astype(jnp.float32) * tails[..., None]).astype(jnp.bfloat16)
    fresh = jnp.einsum(
        "bsgn,bsgrp->bgrnp", write_blocks, tailed, preferred_element_type=jnp.float32
    )
    fresh = gate_ring.settle(fresh)
    gate_ring.advance()
    block_logs = by_head[..., -1].reshape(block_count, group_count, per_group)

    empty_state = jnp.zeros((group_count, per_group, STATE, HEAD), jnp.float32)
    block_decays = jnp.exp(block_logs)
    before, carried = ([], empty_state)
    for block in range(block_count):
        before.append(carried)
        carried = carried * block_decays[block][..., None, None] + fresh[block]
    local_before, local_end = (jnp.stack(before), carried)
    device_decay = jnp.exp(jnp.sum(block_logs, axis=0))

    def packed(decay, state):
        row = jnp.broadcast_to(decay[..., None, None], (*decay.shape, 8, HEAD))
        return jnp.concatenate([state, row], 2)

    def combine(earlier, later):
        decay = later[:, :, STATE : STATE + 1]
        state = earlier[:, :, :STATE] * decay + later[:, :, :STATE]
        return jnp.concatenate([state, earlier[:, :, STATE:] * decay], 2)

    identity = packed(jnp.ones((group_count, per_group), jnp.float32), empty_state)
    incoming = entering_2(packed(device_decay, local_end), "sp", combine, identity)[:, :, :STATE]
    incoming = gate_ring.settle(incoming)
    gate_ring.advance()
    before_block = jnp.cumsum(block_logs, axis=0) - block_logs
    entering_state = local_before + incoming[None] * jnp.exp(before_block)[..., None, None]
    entering = jnp.einsum(
        "blgn,bgrnp->blgrp",
        read_blocks.astype(jnp.float32),
        entering_state,
        precision=lax.Precision.HIGHEST,
    )
    entering = (
        entering * jnp.exp(running).reshape(block_count, BLOCK, group_count, per_group)[..., None]
    )
    mixer = (inside + entering).reshape(row_count, head_count * HEAD)
    gated = (mixer * jax.nn.silu(output_gate_projected.astype(jnp.float32))).reshape(
        row_count, group_count, -1
    )
    gated = gated * lax.rsqrt(jnp.mean(gated * gated, axis=-1, keepdims=True) + epsilon)
    normed = (gated.reshape(row_count, -1) * gated_group_norm_gain).astype(jnp.bfloat16)
    share = row_count // lax.axis_size("tp")
    tp_index = lax.axis_index("tp")
    normed = gate_ring.settle(normed)
    gate_ring.advance()
    summed = product_scattered(normed, mixer_output_weight, "tp")
    own_residual = lax.dynamic_slice_in_dim(residual, tp_index * share, share, 0)
    stream = (own_residual.astype(jnp.float32) + summed).astype(jnp.bfloat16)
    ffn_rows = rows_gathered(channel_norm(stream, feedforward_norm_gain), "tp")
    gate_rest = lax.all_gather(feedforward_gate_weight[:, by_ring:], "sp", axis=0, tiled=True)
    value_full = lax.all_gather(feedforward_value_weight, "sp", axis=0, tiled=True)
    gate_full = jnp.concatenate([gate_ring.gathered(), gate_rest], 1)
    gate_sum = jnp.dot(ffn_rows, gate_full, preferred_element_type=jnp.float32)
    value_sum = jnp.dot(ffn_rows, value_full, preferred_element_type=jnp.float32)
    gate_rows = gate_sum.astype(jnp.bfloat16)
    value_rows = value_sum.astype(jnp.bfloat16)
    ffn_rim = gate_filter_taps.shape[0] - 1
    rim_gate, rim_value = from_behind(
        (gate_rows[row_count - ffn_rim :], value_rows[row_count - ffn_rim :]), "sp", 1
    )
    hidden = (
        jax.nn.silu(causal_taps(gate_rows, rim_gate, gate_filter_taps))
        * causal_taps(value_rows, rim_value, single_value_filter_taps)
    ).astype(jnp.bfloat16)
    down_full = lax.all_gather(feedforward_down_weight, "sp", axis=1, tiled=True)
    down = product_scattered(hidden, down_full, "tp")
    return (stream.astype(jnp.float32) + down).astype(jnp.bfloat16)


MESH = pl.DeviceIdType.MESH
LANE = 128
RIM = 16
F32, BF16 = jnp.float32, jnp.bfloat16


def matmul(a, b):
    return jnp.dot(a, b, preferred_element_type=F32)


def silu(v):
    return v / (1.0 + jnp.exp(-v))


def head_lanes(columns, per_tile, rows):
    lane = lax.broadcasted_iota(jnp.int32, (rows, LANE), 1)
    tiles = []
    for first in range(0, columns.shape[1], per_tile):
        tile = jnp.broadcast_to(columns[:, first : first + 1], (rows, LANE))
        for k in range(1, per_tile):
            other = jnp.broadcast_to(columns[:, first + k : first + k + 1], (rows, LANE))
            tile = jnp.where(lane < k * HEAD, tile, other)
        tiles.append(tile)
    return tiles


def fused_kernel(nsp, ntp, dims, *refs):
    (R, CH, NH, D, F, FS, KS, SH) = dims
    (
        xv, rw, og, steps, vtaps, rwtaps, ggain, wout, resid, fgain, gw, vw, gtaps, staps, dw,
        out,
        halo_x, halo_rw, xf, rwf, scaled, rwc, rwT, cumT_s, cum_s, before, blog, inside, msg, win, got,
        incoming, normed, psend, pgot, xsend, xgot, own_sum, res, stream,
        gst, vst, dst, gfull, vfull, dfull, X, gs, vs, hidden, osend, cgot, r1got, r2send, r2got, own_down,
        ssem, rsem, lsem,
    ) = refs
    Z = nsp // 2
    NB = R // BLOCK
    NT = CH // LANE
    PER = LANE // HEAD
    OFF = F - FS
    s, t = lax.axis_index("sp"), lax.axis_index("tp")
    z, y = s // 2, s % 2
    zl = z % 2
    x, c = t // 2, t % 2
    s_z = s + 2 - 4 * zl
    s_y = s + 1 - 2 * y
    t_c = t + 1 - 2 * c
    t_x = (t + 2) % 4
    P_c, P_x, P_z, P_y = (s, t_c), (s, t_x), (s_z, t), (s_y, t)

    counter = [0]
    pending = []

    def ids(n=1):
        first = counter[0]
        counter[0] += n
        return first

    def rcopy(src, dest, i, device):
        return pltpu.make_async_remote_copy(
            src_ref=src, dst_ref=dest, send_sem=ssem.at[i], recv_sem=rsem.at[i],
            device_id=device, device_id_type=MESH,
        )

    def send(src, dest, i, device, cond=None):
        def go():
            rcopy(src, dest, i, device).start()

        def done():
            rcopy(src, dest, i, device).wait_send()

        if cond is None:
            go()
            pending.append(done)
        else:
            pl.when(cond)(go)
            pending.append(lambda: pl.when(cond)(done))

    def recv(dest, i, cond=None):
        def go():
            rcopy(dest, dest, i, P_c).wait_recv()

        if cond is None:
            go()
        else:
            pl.when(cond)(go)

    own_w, stage, full = (gw, vw, dw), (gst, vst, dst), (gfull, vfull, dfull)
    hop_id = [[[ids() for _ in range(Z)] for _ in range(2)] for _ in range(3)]
    y_id = [[ids() for _ in range(2 * Z)] for _ in range(3)]
    local_n = [0]
    local_done = [[] for _ in range(3)]
    y_wait = [[] for _ in range(3)]

    def part(m, ref, start, size):
        if m < 2:
            return ref.at[:, pl.ds(start, size)]
        return ref.at[pl.ds(start, size), :]

    def place(m, shard):
        first = pl.multiple_of((2 * shard + y) * KS, KS)
        if m < 2:
            return full[m].at[pl.ds(first, KS), :]
        return full[m].at[:, pl.ds(first, KS)]

    def forward(m, k):
        for up in (True, False):
            shard = z - (k - 1) if up else z + (k - 1)
            to = s + 2 if up else s - 2
            src = own_w[m] if k == 1 else stage[m].at[shard]
            dest = stage[m].at[shard]
            i = hop_id[m][0 if up else 1][k]
            have = (z >= k - 1) if up else (z <= Z - k)
            if up:
                long, short = have & (z < Z - 2), have & (z == Z - 2)
                start = ((Z - 1) % 2) * OFF
            else:
                long, short = have & (z > 1), have & (z == 1)
                start = 0
            send(src, dest, i, (to, t), long)
            send(part(m, src, start, FS), part(m, dest, start, FS), i, (to, t), short)

    def deliver(m, shard, src, slot, cond):
        mine = pl.multiple_of(zl * OFF, LANE)
        piece = part(m, src, mine, FS)
        target = place(m, shard)
        send(piece, target, y_id[m][slot], P_y, cond)
        n = local_n[0]
        local_n[0] += 1
        local = pltpu.make_async_copy(piece, target, lsem.at[n])
        if cond is None:
            local.start()
            local_done[m].append(local.wait)
            y_wait[m].append(lambda: recv(target, y_id[m][slot]))
        else:
            pl.when(cond)(lambda: local.start())
            local_done[m].append(lambda: pl.when(cond)(lambda: local.wait()))
            y_wait[m].append(lambda: recv(target, y_id[m][slot], cond))

    def service(m, k):
        for up in (True, False):
            i = hop_id[m][0 if up else 1][k]
            shard = z - k if up else z + k
            have = (z >= k) if up else (z <= Z - 1 - k)
            edge = (z == Z - 1) if up else (z == 0)
            start = ((Z - 1) % 2) * OFF if up else 0
            dest = stage[m].at[shard]
            recv(dest, i, have & jnp.logical_not(edge))
            recv(part(m, dest, start, FS), i, have & edge)
        if k + 1 < Z:
            forward(m, k + 1)
        for up in (True, False):
            shard = z - k if up else z + k
            have = (z >= k) if up else (z <= Z - 1 - k)
            deliver(m, shard, stage[m].at[shard], k if up else Z - 1 + k, have)

    def begin(m):
        forward(m, 1)
        deliver(m, z, own_w[m], 0, None)

    def ready(m):
        for f in local_done[m]:
            f()
        for f in y_wait[m]:
            f()

    i_hx, i_hr = ids(), ids()
    send(xv.at[pl.ds(R - RIM, RIM), :], halo_x, i_hx, (s + 1, t), s < nsp - 1)
    send(rw.at[pl.ds(R - RIM, RIM), :], halo_rw, i_hr, (s + 1, t), s < nsp - 1)
    begin(0)
    res_copy = pltpu.make_async_copy(
        resid.at[pl.ds(pl.multiple_of(t * SH, SH), SH), :], res, lsem.at[lsem.shape[0] - 1]
    )
    res_copy.start()

    @pl.when(s == 0)
    def _():
        halo_x[...] = jnp.zeros_like(halo_x)
        halo_rw[...] = jnp.zeros_like(halo_rw)

    xf[8:, :] = xv[...].astype(F32)
    rwf[8:, :] = rw[...].astype(F32)
    recv(halo_x, i_hx, s > 0)
    recv(halo_rw, i_hr, s > 0)
    xf[:8, :] = halo_x[...].astype(F32)[RIM - 8 :]
    rwf[:8, :] = halo_rw[...].astype(F32)[RIM - 8 :]

    vt, rt = vtaps[...].astype(F32), rwtaps[...].astype(F32)
    K = vt.shape[0]
    row = lax.broadcasted_iota(jnp.int32, (BLOCK, BLOCK), 0)
    col = lax.broadcasted_iota(jnp.int32, (BLOCK, BLOCK), 1)
    upper = (row <= col).astype(F32)
    carried = jnp.zeros((STATE, CH), F32)
    total = jnp.zeros((1, NH), F32)
    for b in range(NB):
        at = slice(b * BLOCK, (b + 1) * BLOCK)
        step_t = steps[0:NH, at]
        cum_t = jnp.dot(
            steps[NH : 2 * NH, at], upper, preferred_element_type=F32,
            precision=lax.Precision.HIGHEST,
        )
        step, cum = step_t.T, cum_t.T
        cumT_s[:, at] = cum_t
        cum_s[at, :] = cum
        last = cum[BLOCK - 1 : BLOCK, :]
        tails = head_lanes(jnp.exp(last - cum), PER, BLOCK)
        step_tiles = head_lanes(step, PER, BLOCK)
        rw_conv = jnp.zeros((BLOCK, rwf.shape[1]), F32)
        for j in range(K):
            start = 8 - (K - 1) + j + b * BLOCK
            rw_conv = rw_conv + rt[j : j + 1, :] * rwf[start : start + BLOCK, :]
        rw_conv = silu(rw_conv)
        rwc[at, :] = rw_conv.astype(BF16)
        turned = rw_conv.T.astype(BF16)
        rwT[b] = turned
        parts = []
        for p in range(NT):
            lanes = slice(p * LANE, (p + 1) * LANE)
            conv = jnp.zeros((BLOCK, LANE), F32)
            for j in range(K):
                start = 8 - (K - 1) + j + b * BLOCK
                conv = conv + vt[j : j + 1, lanes] * xf[start : start + BLOCK, lanes]
            conv = silu(conv).astype(BF16).astype(F32)
            value = (conv * step_tiles[p]).astype(BF16)
            scaled[at, lanes] = value
            parts.append((value.astype(F32) * tails[p]).astype(BF16))
        fresh = matmul(turned[STATE:], jnp.concatenate(parts, 1))
        before[b] = carried
        blog[b : b + 1, 0:NH] = total
        decay = jnp.concatenate(head_lanes(jnp.exp(last), PER, 1), 1)
        carried = carried * decay + fresh
        total = total + last
    msg[0:STATE, :] = carried
    msg[STATE:, :] = jnp.broadcast_to(
        jnp.concatenate(head_lanes(jnp.exp(total), PER, 1), 1), (8, CH)
    )

    def shift(source, slot, i, by):
        send(source, got.at[slot], i, (s + by, t), s + by < nsp)

    def arrived(slot, i, by):
        recv(got.at[slot], i, s >= by)

        @pl.when(s < by)
        def _():
            got[slot, 0:STATE, :] = jnp.zeros((STATE, CH), F32)
            got[slot, STATE:, :] = jnp.ones((8, CH), F32)

    def join(earlier, later):
        decay = later[STATE : STATE + 1, :]
        state = earlier[0:STATE, :] * decay + later[0:STATE, :]
        return jnp.concatenate([state, earlier[STATE:, :] * decay], 0)

    widths = []
    width = 1
    while width < nsp - 1:
        widths.append(2 if width == 1 else width)
        width *= 2
    scan_ids = [ids() for _ in range(len(widths) + 1)]
    shift(msg, 0, scan_ids[0], 1)
    shift(msg, 1, scan_ids[1], 2)
    begin(1)

    causal = row >= col
    lane_b = lax.broadcasted_iota(jnp.int32, (BLOCK, LANE), 1)

    def inside_block(b):
        at = slice(b * BLOCK, (b + 1) * BLOCK)
        scores = matmul(rwc[at, 0:STATE], rwT[b, STATE:, :])
        cum, cum_t = cum_s[at, :], cumT_s[:, at]
        for p in range(NT):
            lanes = slice(p * LANE, (p + 1) * LANE)
            value = scaled[at, lanes].astype(F32)
            left, right = [], []
            for k in range(PER):
                h = p * PER + k
                spread = cum[:, h : h + 1] - cum_t[h : h + 1, :]
                left.append((scores * jnp.exp(jnp.where(causal, spread, -jnp.inf))).astype(BF16))
                mine = (lane_b >= k * HEAD) & (lane_b < (k + 1) * HEAD)
                right.append(jnp.where(mine, value, 0.0).astype(BF16))
            inside[at, lanes] = matmul(jnp.concatenate(left, 1), jnp.concatenate(right, 0))

    third = (NB + 2) // 3
    for b in range(0, third):
        inside_block(b)
    arrived(0, scan_ids[0], 1)
    arrived(1, scan_ids[1], 2)
    win[0] = join(got[1], got[0])
    done_blocks, w = third, 0
    for r, by in enumerate(widths[1:]):
        shift(win.at[w], r + 2, scan_ids[r + 2], by)
        for b in range(done_blocks, min(NB, done_blocks + third)):
            inside_block(b)
        done_blocks = min(NB, done_blocks + third)
        if r == 0:
            service(0, 1)
        arrived(r + 2, scan_ids[r + 2], by)
        win[w + 1] = join(got[r + 2], win[w])
        w += 1
    for b in range(done_blocks, NB):
        inside_block(b)
    entering = win[w, 0:STATE, :]

    for b in range(NB):
        at = slice(b * BLOCK, (b + 1) * BLOCK)
        fade = jnp.concatenate(head_lanes(jnp.exp(blog[b : b + 1, 0:NH]), PER, 1), 1)
        state = before[b] + entering * fade
        high = state.astype(BF16)
        low = (state - high.astype(F32)).astype(BF16)
        read = rwc[at, 0:STATE]
        enter = matmul(read, high) + matmul(read, low)
        grown = jnp.concatenate(head_lanes(jnp.exp(cum_s[at, :]), PER, BLOCK), 1)
        gated = (inside[at, :] + enter * grown) * silu(og[at, :].astype(F32))
        scale = lax.rsqrt(jnp.mean(gated * gated, axis=-1, keepdims=True) + epsilon)
        normed[at, :] = (gated * scale * ggain[...]).astype(BF16)

    NCH = 512
    i_p = [ids(), ids()]
    i_x = ids()

    def rows_of(index):
        return pl.ds(pl.multiple_of(index * SH, SH), SH)

    for k, target in enumerate(((t_c + 2) % 4, t_c)):
        for n in range(0, D, NCH):
            psend[k, :, n : n + NCH] = matmul(
                normed[rows_of(target), :], wout[:, n : n + NCH]
            ).astype(BF16)
        send(psend.at[k], pgot.at[k], i_p[k], P_c)
    recv(pgot.at[0], i_p[0])
    for n in range(0, D, NCH):
        xsend[:, n : n + NCH] = (
            matmul(normed[rows_of(t_x), :], wout[:, n : n + NCH])
            + pgot[0, :, n : n + NCH].astype(F32)
        ).astype(BF16)
    send(xsend, xgot, i_x, P_x)
    res_copy.wait()
    recv(pgot.at[1], i_p[1])
    for n in range(0, D, NCH):
        own_sum[:, n : n + NCH] = (
            matmul(normed[rows_of(t), :], wout[:, n : n + NCH])
            + pgot[1, :, n : n + NCH].astype(F32)
            + res[:, n : n + NCH].astype(F32)
        )
    service(1, 1)
    begin(2)
    recv(xgot, i_x)
    RC = 16
    for r in range(0, SH, RC):
        part_sum = own_sum[r : r + RC, :] + xgot[r : r + RC, :].astype(F32)
        kept = part_sum.astype(BF16)
        stream[r : r + RC, :] = kept
        floats = kept.astype(F32)
        scale = lax.rsqrt(jnp.mean(floats * floats, axis=-1, keepdims=True) + epsilon)
        X[zl, pl.ds(pl.multiple_of(RIM + t * SH + r, RC), RC), :] = (
            floats * scale * fgain[...]
        ).astype(BF16)

    HALF = SH // 2

    def rows_at(zi, ti, first=0, size=SH):
        return X.at[zi, pl.ds(pl.multiple_of(RIM + ti * SH + first, RIM), size), :]

    zo = 1 - zl
    i_rim = [ids() for _ in range(2 * ntp)]
    nxt = s + 1
    nz, ny = nxt // 2, nxt % 2
    nzl = nz % 2
    rim_here = rows_at(zl, t, SH - RIM, RIM)
    for a in range(2):
        nz_to = nz if a == 0 else nz + 1 - 2 * nzl
        for ti in range(ntp):
            def go(nz_to=nz_to, ti=ti, j=a * ntp + ti):
                return pltpu.make_async_remote_copy(
                    src_ref=rim_here, dst_ref=X.at[nzl, pl.ds(0, RIM), :],
                    send_sem=ssem.at[i_rim[0] + j], recv_sem=rsem.at[i_rim[0] + nzl],
                    device_id=(2 * nz_to + ny, ti), device_id_type=MESH,
                )

            cond = (t == ntp - 1) & (nxt < nsp)
            pl.when(cond)(lambda go=go: go().start())
            pending.append(lambda go=go, cond=cond: pl.when(cond)(lambda: go().wait_send()))
    i_a = [ids() for _ in range(10)]
    own_rows = rows_at(zl, t)
    send(own_rows, own_rows, i_a[0], P_x)
    send(own_rows, own_rows, i_a[1], P_z)
    send(own_rows, own_rows, i_a[2], P_c)
    service(0, 2)
    service(0, 3)
    recv(rows_at(zl, t_x), i_a[0])
    send(rows_at(zl, t_x, 0, HALF), rows_at(zl, t_x, 0, HALF), i_a[3], P_z)
    send(rows_at(zl, t_x), rows_at(zl, t_x), i_a[4], P_c)
    recv(rows_at(zo, t), i_a[1])
    send(rows_at(zo, t, HALF, HALF), rows_at(zo, t, HALF, HALF), i_a[5], P_x)
    send(rows_at(zo, t), rows_at(zo, t), i_a[6], P_c)
    service(1, 2)
    service(1, 3)
    recv(rows_at(zo, t_x, 0, HALF), i_a[3])
    send(rows_at(zo, t_x, 0, HALF), rows_at(zo, t_x, 0, HALF), i_a[7], P_c)
    recv(rows_at(zo, t_x, HALF, HALF), i_a[5])
    send(rows_at(zo, t_x, HALF, HALF), rows_at(zo, t_x, HALF, HALF), i_a[8], P_c)
    recv(rows_at(zl, t_c), i_a[2])
    recv(rows_at(zl, (t_c + 2) % 4), i_a[4])
    recv(rows_at(zo, t_c), i_a[6])
    for zi in range(2):
        first_block = 2 * (z - zl + zi) + y
        recv(X.at[zi, pl.ds(0, RIM), :], i_rim[0] + zi, first_block > 0)

        @pl.when(first_block == 0)
        def _(zi=zi):
            X[zi, 0:RIM, :] = jnp.zeros((RIM, D), BF16)

    recv(rows_at(zo, (t_c + 2) % 4, 0, HALF), i_a[7])
    recv(rows_at(zo, (t_c + 2) % 4, HALF, HALF), i_a[8])
    service(2, 1)
    ready(0)
    ready(1)

    MC = RIM + R // 2
    NC = 256
    KF = gtaps.shape[0]
    over = 2 * FS - F
    lane_f = lax.broadcasted_iota(jnp.int32, (KF, FS), 1)
    double = (zl == 1) & (lane_f < over)

    def my_taps(ref):
        taps = ref[...].astype(F32)
        taps = jnp.where(zl == 0, taps[:, :FS], taps[:, OFF:])
        return jnp.where(double, 0.0, taps)

    gt, st = my_taps(gtaps), my_taps(staps)

    def one_half(zi, _):
        zc = (zl + zi) % 2

        def chunk(q, _):
            rows = pl.ds(pl.multiple_of(q * (R // 2), RIM), MC)
            for n in range(0, FS, NC):
                here = X[zc, rows, :]
                gs[rows, n : n + NC] = matmul(here, gfull[:, n : n + NC]).astype(BF16).astype(F32)
                vs[rows, n : n + NC] = matmul(here, vfull[:, n : n + NC]).astype(BF16).astype(F32)
            return 0

        lax.fori_loop(0, 2, chunk, 0)
        RB = 64
        for r in range(0, R, RB):
            for n in range(0, FS, NC):
                lanes = slice(n, n + NC)
                gate = jnp.zeros((RB, NC), F32)
                value = jnp.zeros((RB, NC), F32)
                for j in range(KF):
                    start = RIM - (KF - 1) + j + r
                    gate = gate + gt[j : j + 1, lanes] * gs[start : start + RB, lanes]
                    value = value + st[j : j + 1, lanes] * vs[start : start + RB, lanes]
                hidden[zc, r : r + RB, lanes] = (silu(gate) * value).astype(BF16)
        return 0

    lax.fori_loop(0, 2, one_half, 0)
    service(2, 2)
    service(2, 3)
    ready(2)

    i_o = [ids() for _ in range(4)]
    i_r = [ids() for _ in range(4)]
    order = ((zo, 1), (zl, 1), (zo, 0), (zl, 0))

    def down_rows(zi, ti, n):
        return matmul(hidden[zi, pl.ds(pl.multiple_of(ti * SH, SH), SH), :], dfull[:, n : n + NCH])

    for k, (zi, far) in enumerate(order):
        ti = (t_c + 2 * far) % 4
        for n in range(0, D, NCH):
            osend[k, :, n : n + NCH] = down_rows(zi, ti, n).astype(BF16)
        send(osend.at[k], cgot.at[k], i_o[k], P_c)
    recv(cgot.at[0], i_o[0])
    for n in range(0, D, NCH):
        r2send[2, :, n : n + NCH] = (
            down_rows(zo, t_x, n) + cgot[0, :, n : n + NCH].astype(F32)
        ).astype(BF16)
    send(r2send.at[2, pl.ds(0, HALF), :], r1got.at[0], i_r[0], P_x)
    send(r2send.at[2, pl.ds(HALF, HALF), :], r1got.at[1], i_r[1], P_z)
    recv(cgot.at[1], i_o[1])
    for n in range(0, D, NCH):
        own_sum[:, n : n + NCH] = down_rows(zl, t_x, n) + cgot[1, :, n : n + NCH].astype(F32)
    recv(cgot.at[2], i_o[2])
    for n in range(0, D, NCH):
        own_down[:, n : n + NCH] = down_rows(zo, t, n) + cgot[2, :, n : n + NCH].astype(F32)
    recv(r1got.at[1], i_r[1])
    r2send[0, 0:HALF, :] = own_sum[0:HALF, :].astype(BF16)
    r2send[0, HALF:, :] = (own_sum[HALF:, :] + r1got[1].astype(F32)).astype(BF16)
    send(r2send.at[0], r2got.at[0], i_r[2], P_x)
    recv(r1got.at[0], i_r[0])
    r2send[1, 0:HALF, :] = (own_down[0:HALF, :] + r1got[0].astype(F32)).astype(BF16)
    r2send[1, HALF:, :] = own_down[HALF:, :].astype(BF16)
    send(r2send.at[1], r2got.at[1], i_r[3], P_z)
    recv(cgot.at[3], i_o[3])
    for n in range(0, D, NCH):
        own_sum[:, n : n + NCH] = (
            down_rows(zl, t, n)
            + cgot[3, :, n : n + NCH].astype(F32)
            + stream[:, n : n + NCH].astype(F32)
        )
    recv(r2got.at[0], i_r[2])
    recv(r2got.at[1], i_r[3])
    for r in range(0, SH, RC):
        here = slice(r, r + RC)
        out[here, :] = (
            own_sum[here, :] + r2got[0, here, :].astype(F32) + r2got[1, here, :].astype(F32)
        ).astype(BF16)
    for f in pending:
        f()
    assert counter[0] <= ssem.shape[0]
    assert local_n[0] < lsem.shape[0]


def fused_dims(nsp, ntp, args):
    R, CH = args[0].shape
    NH = args[4].shape[1]
    D, F = args[12].shape[1], args[15].shape[1]
    fits = (
        nsp % 4 == 0 and nsp == 8 and ntp == 4
        and args[1].shape[1] == STATE and args[2].shape[1] == STATE
        and NH == 8 and CH == NH * HEAD and 2 * STATE == LANE
        and R % BLOCK == 0 and R % (ntp * 2 * RIM) == 0
        and D % (nsp * LANE) == 0 and D % 512 == 0 and F % LANE == 0
        and args[8].shape[0] <= 8 and args[17].shape[0] <= 8
    )
    FS = (F // LANE + 1) // 2 * LANE
    if not fits or FS % 256:
        return None
    return (R, CH, NH, D, F, FS, D // nsp, R // ntp)


def fused_on_device(nsp, ntp, dims, args):
    (
        xv, write, read, og, scores, extra, bias, rate, vtaps, wtaps, rtaps, ggain, wout, resid,
        fgain, gw, vw, gtaps, staps, dw,
    ) = args
    (R, CH, NH, D, F, FS, KS, SH) = dims
    Z, NB = nsp // 2, R // BLOCK
    step = jax.nn.softplus(scores + bias)
    log_decay = -step * jnp.exp(rate) + extra
    steps = jnp.concatenate([step, log_decay], 1).T
    rw = jnp.concatenate([read, write], 1)
    rwtaps = jnp.concatenate([rtaps, wtaps], 1)
    rounds = max(1, (nsp - 2).bit_length())
    V = pltpu.VMEM
    scratch = [
        V((RIM, CH), BF16), V((RIM, LANE), BF16), V((8 + R, CH), F32), V((8 + R, LANE), F32),
        V((R, CH), BF16), V((R, LANE), BF16), V((NB, LANE, BLOCK), BF16), V((NH, R), F32),
        V((R, NH), F32), V((NB, STATE, CH), F32), V((NB + 2, LANE), F32), V((R, CH), F32),
        V((STATE + 8, CH), F32), V((rounds + 1, STATE + 8, CH), F32),
        V((rounds + 2, STATE + 8, CH), F32),
        V((8, LANE), F32), V((R, CH), BF16), V((2, SH, D), BF16), V((2, SH, D), BF16),
        V((SH, D), BF16), V((SH, D), BF16), V((SH, D), F32), V((SH, D), BF16), V((SH, D), BF16),
        V((Z, KS, F), BF16), V((Z, KS, F), BF16), V((Z, F, KS), BF16),
        V((D, FS), BF16), V((D, FS), BF16), V((FS, D), BF16),
        V((2, RIM + R, D), BF16), V((RIM + R, FS), F32), V((RIM + R, FS), F32),
        V((2, R, FS), BF16), V((4, SH, D), BF16), V((4, SH, D), BF16), V((2, SH // 2, D), BF16),
        V((3, SH, D), BF16), V((2, SH, D), BF16), V((SH, D), F32),
        pltpu.SemaphoreType.DMA((96,)), pltpu.SemaphoreType.DMA((96,)),
        pltpu.SemaphoreType.DMA((32,)),
    ]
    vm, hbm = pl.BlockSpec(memory_space=pltpu.VMEM), pl.BlockSpec(memory_space=pl.ANY)
    return pl.pallas_call(
        functools.partial(fused_kernel, nsp, ntp, dims),
        out_shape=jax.ShapeDtypeStruct((SH, D), BF16),
        in_specs=[vm, vm, vm, vm, vm, vm, vm, vm, hbm, vm, hbm, hbm, vm, vm, hbm],
        out_specs=vm,
        scratch_shapes=scratch,
        compiler_params=pltpu.CompilerParams(
            has_side_effects=True, vmem_limit_bytes=67043328
        ),
    )(
        xv, rw, og, steps, vtaps, rwtaps, ggain.reshape(1, CH), wout, resid, fgain.reshape(1, D),
        gw, vw, gtaps, staps, dw,
    )


def on_device(nsp, ntp, *args):
    dims = fused_dims(nsp, ntp, args)
    if dims is None:
        return plain_on_device(*args)
    return fused_on_device(nsp, ntp, dims, args)


def solution(mesh):
    placed = (
        P("sp", "tp"),
        P("sp", "tp"),
        P("sp", "tp"),
        P("sp", "tp"),
        P("sp", "tp"),
        P("sp", "tp"),
        P("tp"),
        P("tp"),
        P(None, "tp"),
        P(None, "tp"),
        P(None, "tp"),
        P("tp"),
        P("tp", None),
        P("sp", None),
        P(),
        P("sp", "tp"),
        P("sp", "tp"),
        P(None, "tp"),
        P(None, "tp"),
        P("tp", "sp"),
    )
    return jax.shard_map(
        functools.partial(on_device, mesh.shape["sp"], mesh.shape["tp"]), mesh=mesh, in_specs=placed, out_specs=P(("sp", "tp"), None), check_vma=False
    )
```

```python
import functools

import jax
import jax.numpy as jnp
from jax import lax
from jax.experimental import pallas as pl
from jax.experimental.pallas import tpu as pltpu
from jax.sharding import PartitionSpec as P

HEAD = 64
STATE = 64
BLOCK = 128


epsilon = 1e-06


def from_behind(value, axis, by):
    length = lax.axis_size(axis)
    pairs = [(i, i + by) for i in range(length) if 0 <= i + by < length]
    return lax.ppermute(value, axis, pairs)


def entering_2(value, axis, join, neutral):
    count, mine = (lax.axis_size(axis), lax.axis_index(axis))

    def shifted(part, by):
        moved = from_behind(part, axis, by)
        return jnp.where(mine >= by, moved, neutral)

    if count == 1:
        return neutral
    window, width = (shifted(value, 1), 1)
    while width < count - 1:
        earlier = shifted(value, 2) if width == 1 else shifted(window, width)
        window, width = (join(earlier, window), 2 * width)
    return window


def halving_bits(axis):
    count = lax.axis_size(axis)
    return [1 << b for b in range(count.bit_length() - 1)] if count & (count - 1) == 0 else None


def swap(value, axis, bit):
    return lax.ppermute(value, axis, [(i, i ^ bit) for i in range(lax.axis_size(axis))])


def product_scattered(rows, weight, axis):
    count, mine = (lax.axis_size(axis), lax.axis_index(axis))
    bits = halving_bits(axis)
    if not bits:
        product = jnp.dot(rows, weight, preferred_element_type=jnp.float32)
        return lax.psum_scatter(product, axis, scatter_dimension=0, tiled=True)
    share = rows.shape[0] // count

    def side(array, which):
        return lax.dynamic_index_in_dim(
            array.reshape(array.shape[0] // 2, 2, *array.shape[1:]),
            which,
            1,
            keepdims=False,
            allow_negative_indices=False,
        )

    rows = rows.reshape(count, share, -1)

    def multiplied(part):
        flat = jnp.dot(
            part.reshape(-1, part.shape[-1]), weight, preferred_element_type=jnp.float32
        )
        return flat.reshape(part.shape[0], share, -1)

    low = mine & 1
    product = multiplied(rows)
    going = side(product, 1 - low).astype(jnp.bfloat16)
    arrived = swap(going, axis, 1)
    total = side(product, low)
    for bit in bits[1:]:
        own = (mine // bit) & 1
        going = (side(total, 1 - own) + side(arrived, 1 - own).astype(jnp.float32)).astype(
            jnp.bfloat16
        )
        total = side(total, own) + side(arrived, own).astype(jnp.float32)
        arrived = swap(going, axis, bit)
    return (total + arrived.astype(jnp.float32))[0]


def rows_gathered(own, axis):
    bits = halving_bits(axis)
    if not bits:
        return lax.all_gather(own, axis, axis=0, tiled=True)
    mine = lax.axis_index(axis)
    held = own[None]
    for bit in reversed(bits):
        other = swap(held, axis, bit)
        high = ((mine // bit) & 1) == 1
        held = jnp.stack([jnp.where(high, other, held), jnp.where(high, held, other)], 1)
        held = held.reshape(-1, *own.shape)
    return held.reshape(-1, own.shape[-1])


def put(whole, block, index):
    start = (index, *[jnp.zeros_like(index)] * block.ndim)
    return lax.dynamic_update_slice(whole, block[None], start, allow_negative_indices=False)


class RingGather:
    def __init__(self, block, axis):
        self.axis, self.count, self.step = (axis, lax.axis_size(axis), 0)
        count, mine = (self.count, lax.axis_index(axis))
        if count % 2:
            order = list(range(count))
            self.place = mine
        else:
            order = list(range(0, count, 2)) + list(range(count - 1, 0, -2))
            self.place = jnp.where(mine % 2 == 0, mine, 2 * count - 1 - mine) // 2
        self.forward = [(order[p], order[(p + 1) % count]) for p in range(count)]
        self.backward = [(b, a) for a, b in self.forward]
        self.up = self.down = block
        whole = jnp.zeros((count, *block.shape), block.dtype)
        self.whole = put(whole, block, mine)

    def owner(self, place):
        place = lax.rem(place + self.count, self.count)
        if self.count % 2:
            return place
        return jnp.where(2 * place < self.count, 2 * place, 2 * self.count - 1 - 2 * place)

    def advance(self):
        self.step += 1
        if self.step > self.count // 2:
            return
        self.up = lax.ppermute(self.up, self.axis, self.forward)
        self.whole = put(self.whole, self.up, self.owner(self.place - self.step))
        if self.step <= (self.count - 1) // 2:
            self.down = lax.ppermute(self.down, self.axis, self.backward)
            self.whole = put(self.whole, self.down, self.owner(self.place + self.step))

    def settle(self, value):
        value, self.up, self.down = lax.optimization_barrier((value, self.up, self.down))
        return value

    def gathered(self):
        while self.step < self.count // 2:
            self.advance()
        return self.whole.reshape(-1, self.whole.shape[-1])


def causal_taps(current, previous, kernel):
    tap_count = kernel.shape[0]
    length = current.shape[0]
    padded = jnp.concatenate([previous, current], 0).astype(jnp.float32)
    result = jnp.zeros((length, current.shape[1]), jnp.float32)
    for offset in range(tap_count):
        result = result + kernel[offset].astype(jnp.float32) * padded[offset : offset + length]
    return result


def channel_norm(stream, gain):
    floats = stream.astype(jnp.float32)
    scaled = floats * lax.rsqrt(jnp.mean(floats * floats, axis=-1, keepdims=True) + epsilon)
    return (scaled * gain).astype(jnp.bfloat16)


def plain_on_device(
    mixer_value_projection,
    write_vectors_projected,
    read_vectors_projected,
    output_gate_projected,
    step_size_scores,
    position_decay_extra,
    step_size_bias,
    head_decay_logarithm,
    value_filter_taps,
    write_filter_taps,
    read_filter_taps,
    gated_group_norm_gain,
    mixer_output_weight,
    residual,
    feedforward_norm_gain,
    feedforward_gate_weight,
    feedforward_value_weight,
    gate_filter_taps,
    single_value_filter_taps,
    feedforward_down_weight,
):
    row_count = mixer_value_projection.shape[0]
    head_count = step_size_scores.shape[1]
    group_count = write_vectors_projected.shape[1] // STATE
    per_group = head_count // group_count
    mix_rim = value_filter_taps.shape[0] - 1
    channels = (mixer_value_projection.shape[1], write_vectors_projected.shape[1])
    rims = from_behind(
        jnp.concatenate(
            [
                mixer_value_projection[row_count - mix_rim :],
                write_vectors_projected[row_count - mix_rim :],
                read_vectors_projected[row_count - mix_rim :],
            ],
            1,
        ),
        "sp",
        1,
    )
    rim_values, rim_write, rim_read = jnp.split(rims, [channels[0], sum(channels)], axis=1)
    by_ring = feedforward_gate_weight.shape[1] // 256 * 128
    gate_ring = RingGather(feedforward_gate_weight[:, :by_ring], "sp")
    gate_ring.advance()
    x_conv = jax.nn.silu(causal_taps(mixer_value_projection, rim_values, value_filter_taps)).astype(
        jnp.bfloat16
    )
    write_conv = jax.nn.silu(
        causal_taps(write_vectors_projected, rim_write, write_filter_taps)
    ).astype(jnp.bfloat16)
    read_conv = jax.nn.silu(causal_taps(read_vectors_projected, rim_read, read_filter_taps)).astype(
        jnp.bfloat16
    )
    step_size_head = jax.nn.softplus(step_size_scores + step_size_bias)
    logarithm_decay_rate = -step_size_head * jnp.exp(head_decay_logarithm) + position_decay_extra
    scaled = (
        x_conv.astype(jnp.float32).reshape(row_count, head_count, HEAD) * step_size_head[:, :, None]
    ).astype(jnp.bfloat16)
    block_count = row_count // BLOCK
    value_blocks = scaled.reshape(block_count, BLOCK, group_count, per_group, HEAD)
    write_blocks = write_conv.reshape(block_count, BLOCK, group_count, STATE)
    read_blocks = read_conv.reshape(block_count, BLOCK, group_count, STATE)
    running = jnp.cumsum(logarithm_decay_rate.reshape(block_count, BLOCK, head_count), axis=1)
    by_head = jnp.moveaxis(running, 1, 2)
    spread = by_head[..., :, None] - by_head[..., None, :]
    causal = jnp.tril(jnp.ones((BLOCK, BLOCK), dtype=jnp.bool_))
    decays = jnp.exp(jnp.where(causal, spread, -jnp.inf)).reshape(
        block_count, group_count, per_group, BLOCK, BLOCK
    )
    scores = jnp.einsum(
        "blgn,bsgn->bgls", read_blocks, write_blocks, preferred_element_type=jnp.float32
    )
    weights = (scores[:, :, None] * decays).astype(jnp.bfloat16)
    inside = jnp.einsum(
        "bgrls,bsgrp->blgrp", weights, value_blocks, preferred_element_type=jnp.float32
    )
    tails = jnp.moveaxis(jnp.exp(by_head[..., -1:] - by_head), 2, 1).reshape(
        block_count, BLOCK, group_count, per_group
    )
    tailed = (value_blocks.astype(jnp.float32) * tails[..., None]).astype(jnp.bfloat16)
    fresh = jnp.einsum(
        "bsgn,bsgrp->bgrnp", write_blocks, tailed, preferred_element_type=jnp.float32
    )
    fresh = gate_ring.settle(fresh)
    gate_ring.advance()
    block_logs = by_head[..., -1].reshape(block_count, group_count, per_group)

    empty_state = jnp.zeros((group_count, per_group, STATE, HEAD), jnp.float32)
    block_decays = jnp.exp(block_logs)
    before, carried = ([], empty_state)
    for block in range(block_count):
        before.append(carried)
        carried = carried * block_decays[block][..., None, None] + fresh[block]
    local_before, local_end = (jnp.stack(before), carried)
    device_decay = jnp.exp(jnp.sum(block_logs, axis=0))

    def packed(decay, state):
        row = jnp.broadcast_to(decay[..., None, None], (*decay.shape, 8, HEAD))
        return jnp.concatenate([state, row], 2)

    def combine(earlier, later):
        decay = later[:, :, STATE : STATE + 1]
        state = earlier[:, :, :STATE] * decay + later[:, :, :STATE]
        return jnp.concatenate([state, earlier[:, :, STATE:] * decay], 2)

    identity = packed(jnp.ones((group_count, per_group), jnp.float32), empty_state)
    incoming = entering_2(packed(device_decay, local_end), "sp", combine, identity)[:, :, :STATE]
    incoming = gate_ring.settle(incoming)
    gate_ring.advance()
    before_block = jnp.cumsum(block_logs, axis=0) - block_logs
    entering_state = local_before + incoming[None] * jnp.exp(before_block)[..., None, None]
    entering = jnp.einsum(
        "blgn,bgrnp->blgrp",
        read_blocks.astype(jnp.float32),
        entering_state,
        precision=lax.Precision.HIGHEST,
    )
    entering = (
        entering * jnp.exp(running).reshape(block_count, BLOCK, group_count, per_group)[..., None]
    )
    mixer = (inside + entering).reshape(row_count, head_count * HEAD)
    gated = (mixer * jax.nn.silu(output_gate_projected.astype(jnp.float32))).reshape(
        row_count, group_count, -1
    )
    gated = gated * lax.rsqrt(jnp.mean(gated * gated, axis=-1, keepdims=True) + epsilon)
    normed = (gated.reshape(row_count, -1) * gated_group_norm_gain).astype(jnp.bfloat16)
    share = row_count // lax.axis_size("tp")
    tp_index = lax.axis_index("tp")
    normed = gate_ring.settle(normed)
    gate_ring.advance()
    summed = product_scattered(normed, mixer_output_weight, "tp")
    own_residual = lax.dynamic_slice_in_dim(residual, tp_index * share, share, 0)
    stream = (own_residual.astype(jnp.float32) + summed).astype(jnp.bfloat16)
    ffn_rows = rows_gathered(channel_norm(stream, feedforward_norm_gain), "tp")
    gate_rest = lax.all_gather(feedforward_gate_weight[:, by_ring:], "sp", axis=0, tiled=True)
    value_full = lax.all_gather(feedforward_value_weight, "sp", axis=0, tiled=True)
    gate_full = jnp.concatenate([gate_ring.gathered(), gate_rest], 1)
    gate_sum = jnp.dot(ffn_rows, gate_full, preferred_element_type=jnp.float32)
    value_sum = jnp.dot(ffn_rows, value_full, preferred_element_type=jnp.float32)
    gate_rows = gate_sum.astype(jnp.bfloat16)
    value_rows = value_sum.astype(jnp.bfloat16)
    ffn_rim = gate_filter_taps.shape[0] - 1
    rim_gate, rim_value = from_behind(
        (gate_rows[row_count - ffn_rim :], value_rows[row_count - ffn_rim :]), "sp", 1
    )
    hidden = (
        jax.nn.silu(causal_taps(gate_rows, rim_gate, gate_filter_taps))
        * causal_taps(value_rows, rim_value, single_value_filter_taps)
    ).astype(jnp.bfloat16)
    down_full = lax.all_gather(feedforward_down_weight, "sp", axis=1, tiled=True)
    down = product_scattered(hidden, down_full, "tp")
    return (stream.astype(jnp.float32) + down).astype(jnp.bfloat16)


MESH = pl.DeviceIdType.MESH
LANE = 128
RIM = 16
PLAN = {
    "start": ("B0", "B1", "E0", "E1", "E2", "Y0", "Y1", "Y2",),
    "scan1": ("B2", "E3",),
    "scan2": ("Y3", "E4",),
    "scan3": ("B3", "Y4", "E5", "Y5", "E6",),
    "mixer": ("S01", "B4", "Y6", "E7",),
    "project": ("S11", "B5", "Y7",),
    "sum0": ("S21", "B6", "S02", "S31",),
    "sum1": ("S12", "S41", "B7", "S03",),
    "gather0": ("S51", "S22", "S61", "S32", "S13",),
    "gather1": ("S71", "B8", "S42", "S23",),
    "gather2": ("S52", "S33", "S62", "B9", "S43", "S72", "E8", "S53", "S63", "E9", "S73", "Y8", "Y9",),
    "ready": (),
    "ffn": ("S81",),
    "conv0": ("S91",),
    "halves": (),
    "conv1": ("S82",),
    "down0": (),
    "down1": ("S92", "S83",),
    "down2": ("S93",),
    "down3": (),
}
F32, BF16 = jnp.float32, jnp.bfloat16


def matmul(a, b):
    return jnp.dot(a, b, preferred_element_type=F32)


def silu(v):
    half = 0.5 * v
    return half + half * jnp.tanh(half)


def head_lanes(columns, per_tile, rows):
    lane = lax.broadcasted_iota(jnp.int32, (rows, LANE), 1)
    tiles = []
    for first in range(0, columns.shape[1], per_tile):
        tile = jnp.broadcast_to(columns[:, first : first + 1], (rows, LANE))
        for k in range(1, per_tile):
            other = jnp.broadcast_to(columns[:, first + k : first + k + 1], (rows, LANE))
            tile = jnp.where(lane < k * HEAD, tile, other)
        tiles.append(tile)
    return tiles


def fused_kernel(nsp, ntp, dims, *refs):
    (R, CH, NH, D, F, FS, KS, SH) = dims
    (
        xv, wT, rT, og_in, scT, exT, bias, rate, vtaps, wtaps, rtaps, ggain, wout_in, resid, fgain,
        gw, vw, gtaps, staps, dw,
        out,
        xin, og, wout, halo_x, halo_rw, xf, rwf, scaled, rwc, rwT, steps, cumT_s, cum_s, before, blog,
        inside, msg, winf, win, got,
        normed, psend, pgot, xsend, xgot, own_sum, res, stream,
        gst, vst, dst, gfull, vfull, dfull, X, gs, vs, hidden, osend, cgot, r1got, r2send, r2got,
        bx_sum, bz_sum,
        ssem, rsem, lsem,
    ) = refs
    Z = nsp // 2
    NB = R // BLOCK
    NT = CH // LANE
    PER = LANE // HEAD
    FA = F - FS
    s, t = lax.axis_index("sp"), lax.axis_index("tp")
    z, y = s // 2, s % 2
    zl, zh = z % 2, z // 2
    x, c = t // 2, t % 2
    outer = (z % 4) * (3 - z % 4) == 0
    inner = jnp.logical_not(outer)
    s_z = s + 2 - 4 * zl
    s_y = s + 1 - 2 * y
    t_c = t + 1 - 2 * c
    t_x = (t + 2) % 4
    P_c, P_x, P_z, P_y = (s, t_c), (s, t_x), (s_z, t), (s_y, t)

    barrier = pltpu.get_barrier_semaphore()
    for i in range(nsp):
        for j in range(ntp):
            @pl.when((s != i) | (t != j))
            def _(i=i, j=j):
                pl.semaphore_signal(barrier, inc=1, device_id=(i, j), device_id_type=MESH)

    pl.semaphore_wait(barrier, nsp * ntp - 1)
    counter = [0]
    pending = []
    scope = [None]

    def mark(name):
        if scope[0] is not None:
            scope[0].__exit__(None, None, None)
        scope[0] = jax.named_scope(name) if name else None
        if name:
            scope[0].__enter__()

    def ids(n=1):
        first = counter[0]
        counter[0] += n
        return first

    def rcopy(src, dest, i, device):
        return pltpu.make_async_remote_copy(
            src_ref=src, dst_ref=dest, send_sem=ssem.at[i], recv_sem=rsem.at[i],
            device_id=device, device_id_type=MESH,
        )

    def send(src, dest, i, device, cond=None):
        def go():
            rcopy(src, dest, i, device).start()

        def done():
            rcopy(src, dest, i, device).wait_send()

        if cond is None:
            go()
            pending.append(done)
        else:
            pl.when(cond)(go)
            pending.append(lambda: pl.when(cond)(done))

    def recv(dest, i, cond=None):
        def go():
            rcopy(dest, dest, i, P_c).wait_recv()

        if cond is None:
            go()
        else:
            pl.when(cond)(go)

    own_w, stage, full = (gw, vw, dw), (gst, vst, dst), (gfull, vfull, dfull)
    cuts = [(m, h, (4, 4, 2)[m]) for m in range(3) for h in range((4, 4, 2)[m])]
    NQ = len(cuts)
    hop_id = [[[ids() for _ in range(Z)] for _ in range(2)] for _ in cuts]
    y_id = [[ids() for _ in range(2 * Z)] for _ in cuts]
    local_n = [0]
    landed = [[] for _ in range(3)]

    def part(q, ref, start, size):
        m, h, n = cuts[q]
        step_q = KS // n
        if m < 2:
            return ref.at[pl.ds(h * step_q, step_q), pl.ds(start, size)]
        return ref.at[pl.ds(start, size), pl.ds(h * step_q, step_q)]

    def place(q, shard):
        m, h, n = cuts[q]
        step_q = KS // n
        if m < 2:
            return full[m].at[pl.ds(pl.multiple_of((2 * shard + y) * KS + h * step_q, step_q), step_q), :]
        near = (2 * (shard % 2) + y) * step_q
        return full[m].at[shard // 2, h, :, pl.ds(pl.multiple_of(near, step_q), step_q)]

    def forward(q, k, inward=True, outward=True):
        m = cuts[q][0]
        for up in (True, False):
            shard = z - (k - 1) if up else z + (k - 1)
            to = s + 2 if up else s - 2
            src = own_w[m] if k == 1 else stage[m].at[shard]
            dest = stage[m].at[shard]
            i = hop_id[q][0 if up else 1][k]
            have = (z >= k - 1) if up else (z <= Z - k)
            if up:
                long, short = have & (z < Z - 2), have & (z == Z - 2)
            else:
                long, short = have & (z > 1), have & (z == 1)
            if inward:
                send(part(q, src, 0, F), part(q, dest, 0, F), i, (to, t), long)
            if outward:
                send(part(q, src, 0, FA), part(q, dest, 0, FA), i, (to, t), short)

    def head_of(q, ref, size):
        if cuts[q][0] < 2:
            return ref.at[:, pl.ds(0, size)]
        return ref.at[pl.ds(0, size), :]

    def both(a, b):
        return a if b is None else (b if a is None else a & b)

    def deliver(q, shard, src, slot, cond, group):
        m = cuts[q][0]
        target = place(q, shard)
        i = y_id[q][slot]
        n = local_n[0]
        local_n[0] += 1
        kinds = []
        for kind, start, size in ((outer, 0, FA), (inner, FA, FS)):
            when = both(cond, kind)
            piece, landing = part(q, src, start, size), head_of(q, target, size)
            send(piece, landing, i, P_y, when)
            local = pltpu.make_async_copy(piece, landing, lsem.at[n])
            pl.when(when)(lambda local=local: local.start())
            kinds.append((when, local, landing))

        def wait(extra=None):
            for when, local, landing in kinds:
                def go(local=local, landing=landing):
                    local.wait()
                    rcopy(landing, landing, i, P_c).wait_recv()

                pl.when(both(when, extra))(go)

        landed[m].append((wait, group, cuts[q][1]))

    def service(q, k):
        m = cuts[q][0]
        for up in (True, False):
            i = hop_id[q][0 if up else 1][k]
            shard = z - k if up else z + k
            have = (z >= k) if up else (z <= Z - 1 - k)
            edge = (z == Z - 1) if up else (z == 0)
            dest = stage[m].at[shard]
            recv(part(q, dest, 0, F), i, have & jnp.logical_not(edge))
            recv(part(q, dest, 0, FA), i, have & edge)
        if k + 1 < Z:
            forward(q, k + 1)
        for up in (True, False):
            shard = z - k if up else z + k
            have = (z >= k) if up else (z <= Z - 1 - k)
            near = (shard // 2) == zh
            deliver(q, shard, stage[m].at[shard], k if up else Z - 1 + k, have, near)

    def ready(m, near=None, piece=None):
        for wait, group, h in landed[m]:
            if near is None:
                wait()
            elif h == piece:
                if group is not None:
                    wait(group if near else jnp.logical_not(group))
                elif near:
                    wait()

    moves = []

    def pump(stop):
        for move in PLAN[stop]:
            assert move not in moves
            moves.append(move)
            q = int(move[1])
            if move[0] == "B":
                forward(q, 1, outward=False)
            elif move[0] == "E":
                forward(q, 1, inward=False)
            elif move[0] == "Y":
                deliver(q, z, own_w[cuts[q][0]], 0, None, None)
            else:
                service(q, int(move[2]))

    mark("rims")
    i_hx, i_hr = ids(), [ids(), ids()]
    send(xv.at[pl.ds(R - RIM, RIM), :], halo_x, i_hx, (s + 1, t), s < nsp - 1)
    send(rT.at[:, pl.ds(R - LANE, LANE)], halo_rw.at[0], i_hr[0], (s + 1, t), s < nsp - 1)
    send(wT.at[:, pl.ds(R - LANE, LANE)], halo_rw.at[1], i_hr[1], (s + 1, t), s < nsp - 1)
    NL = lsem.shape[0]
    x_copy = pltpu.make_async_copy(xv, xin, lsem.at[NL - 1])
    og_copy = pltpu.make_async_copy(og_in, og, lsem.at[NL - 2])
    wout_copy = pltpu.make_async_copy(wout_in, wout, lsem.at[NL - 3])
    res_copy = pltpu.make_async_copy(
        resid.at[pl.ds(pl.multiple_of(t * SH, SH), SH), :], res, lsem.at[NL - 4]
    )
    x_copy.start()
    pump("start")
    og_copy.start()
    wout_copy.start()
    res_copy.start()

    @pl.when(outer)
    def _():
        gfull[:, FA:] = jnp.zeros((D, FS - FA), BF16)
        vfull[:, FA:] = jnp.zeros((D, FS - FA), BF16)
        dfull[:, :, FA:, :] = jnp.zeros((2, 2, FS - FA, D // 4), BF16)

    @pl.when(s == 0)
    def _():
        halo_x[...] = jnp.zeros_like(halo_x)
        halo_rw[...] = jnp.zeros_like(halo_rw)

    eye = lax.broadcasted_iota(jnp.int32, (NH, NH), 0) == lax.broadcasted_iota(jnp.int32, (NH, NH), 1)

    def column(ref):
        return jnp.sum(jnp.where(eye, jnp.broadcast_to(ref[...], (NH, NH)), 0.0), 1, keepdims=True)

    raw = scT[...] + column(bias)
    soft = jnp.maximum(raw, 0.0) + jnp.log1p(jnp.exp(-jnp.abs(raw)))
    steps[0:NH, :] = soft
    steps[NH : 2 * NH, :] = exT[...] - soft * jnp.exp(column(rate))

    def pair(first, second):
        return jnp.concatenate([first.astype(F32), second.astype(F32)], 0).T

    for b in range(NB):
        at = slice(b * BLOCK, (b + 1) * BLOCK)
        rwf[8 + b * BLOCK : 8 + (b + 1) * BLOCK, :] = pair(rT[:, at], wT[:, at])
    x_copy.wait()
    xf[8:, :] = xin[...].astype(F32)
    recv(halo_x, i_hx, s > 0)
    recv(halo_rw.at[0], i_hr[0], s > 0)
    recv(halo_rw.at[1], i_hr[1], s > 0)
    xf[:8, :] = halo_x[...].astype(F32)[RIM - 8 :]
    rwf[:8, :] = pair(halo_rw[0], halo_rw[1])[LANE - 8 :]

    mark("convs")
    vt = vtaps[...].astype(F32)
    rt = jnp.concatenate([rtaps[...].astype(F32), wtaps[...].astype(F32)], 1)
    K = vt.shape[0]
    row = lax.broadcasted_iota(jnp.int32, (BLOCK, BLOCK), 0)
    col = lax.broadcasted_iota(jnp.int32, (BLOCK, BLOCK), 1)
    upper = (row <= col).astype(F32)
    carried = jnp.zeros((STATE, CH), F32)
    total = jnp.zeros((1, NH), F32)
    for b in range(NB):
        at = slice(b * BLOCK, (b + 1) * BLOCK)
        step_t = steps[0:NH, at]
        cum_t = jnp.dot(
            steps[NH : 2 * NH, at], upper, preferred_element_type=F32,
            precision=lax.Precision.HIGHEST,
        )
        step, cum = step_t.T, cum_t.T
        cumT_s[:, at] = cum_t
        cum_s[at, :] = cum
        last = cum[BLOCK - 1 : BLOCK, :]
        tails = head_lanes(jnp.exp(last - cum), PER, BLOCK)
        step_tiles = head_lanes(step, PER, BLOCK)
        rw_conv = jnp.zeros((BLOCK, rwf.shape[1]), F32)
        for j in range(K):
            start = 8 - (K - 1) + j + b * BLOCK
            rw_conv = rw_conv + rt[j : j + 1, :] * rwf[start : start + BLOCK, :]
        rw_conv = silu(rw_conv)
        rwc[at, :] = rw_conv.astype(BF16)
        turned = rw_conv.T.astype(BF16)
        rwT[b] = turned
        parts = []
        for p in range(NT):
            lanes = slice(p * LANE, (p + 1) * LANE)
            conv = jnp.zeros((BLOCK, LANE), F32)
            for j in range(K):
                start = 8 - (K - 1) + j + b * BLOCK
                conv = conv + vt[j : j + 1, lanes] * xf[start : start + BLOCK, lanes]
            conv = silu(conv).astype(BF16).astype(F32)
            value = (conv * step_tiles[p]).astype(BF16)
            scaled[at, lanes] = value
            parts.append((value.astype(F32) * tails[p]).astype(BF16))
        fresh = matmul(turned[STATE:], jnp.concatenate(parts, 1))
        before[b] = carried
        blog[b : b + 1, 0:NH] = total
        decay = jnp.concatenate(head_lanes(jnp.exp(last), PER, 1), 1)
        carried = carried * decay + fresh
        total = total + last

    def pack(ref, state, decay):
        ref[0:STATE, :] = state.astype(BF16)
        high = decay.astype(BF16)
        ref[STATE : STATE + 8, :] = jnp.broadcast_to(high, (8, CH))
        ref[STATE + 8 :, :] = jnp.broadcast_to((decay - high.astype(F32)).astype(BF16), (8, CH))

    pack(msg, carried, jnp.concatenate(head_lanes(jnp.exp(total), PER, 1), 1))

    mark("scan")

    def shift(source, slot, i, by):
        send(source, got.at[slot], i, (s + by, t), s + by < nsp)

    def arrived(slot, i, by):
        recv(got.at[slot], i, s >= by)

        @pl.when(s < by)
        def _():
            got[slot, 0:STATE, :] = jnp.zeros((STATE, CH), BF16)
            got[slot, STATE : STATE + 8, :] = jnp.ones((8, CH), BF16)
            got[slot, STATE + 8 :, :] = jnp.zeros((8, CH), BF16)

    def unpack(ref):
        tail = ref[STATE:, :].astype(F32)
        return ref[0:STATE, :].astype(F32), tail[0:1] + tail[8:9]

    def join(earlier, later):
        return earlier[0] * later[1] + later[0], earlier[1] * later[1]

    widths = []
    width = 1
    while width < nsp - 1:
        widths.append(2 if width == 1 else width)
        width *= 2
    scan_ids = [ids() for _ in range(len(widths) + 1)]
    shift(msg, 0, scan_ids[0], 1)
    shift(msg, 1, scan_ids[1], 2)
    pump("scan1")

    causal = row >= col
    lane_b = lax.broadcasted_iota(jnp.int32, (BLOCK, LANE), 1)

    def inside_block(b):
        at = slice(b * BLOCK, (b + 1) * BLOCK)
        scores = matmul(rwc[at, 0:STATE], rwT[b, STATE:, :])
        cum, cum_t = cum_s[at, :], cumT_s[:, at]
        for p in range(NT):
            lanes = slice(p * LANE, (p + 1) * LANE)
            value = scaled[at, lanes].astype(F32)
            left, right = [], []
            for k in range(PER):
                h = p * PER + k
                spread = cum[:, h : h + 1] - cum_t[h : h + 1, :]
                left.append((scores * jnp.exp(jnp.where(causal, spread, -jnp.inf))).astype(BF16))
                mine = (lane_b >= k * HEAD) & (lane_b < (k + 1) * HEAD)
                right.append(jnp.where(mine, value, 0.0).astype(BF16))
            inside[at, lanes] = matmul(jnp.concatenate(left, 1), jnp.concatenate(right, 0))

    third = (NB + 2) // 3
    for b in range(0, third):
        inside_block(b)
    mark("scan1")
    arrived(0, scan_ids[0], 1)
    arrived(1, scan_ids[1], 2)
    window = join(unpack(got.at[1]), unpack(got.at[0]))
    done_blocks = third
    for r, by in enumerate(widths[1:]):
        pack(win.at[r], *window)
        winf[0:STATE, :] = window[0]
        winf[STATE:, :] = jnp.broadcast_to(window[1], (8, CH))
        shift(win.at[r], r + 2, scan_ids[r + 2], by)
        pump(f"scan{r + 2}")
        for b in range(done_blocks, min(NB, done_blocks + third)):
            inside_block(b)
        done_blocks = min(NB, done_blocks + third)
        mark(f"scan{r + 2}")
        arrived(r + 2, scan_ids[r + 2], by)
        window = join(unpack(got.at[r + 2]), (winf[0:STATE, :], winf[STATE : STATE + 1, :]))
    for b in range(done_blocks, NB):
        inside_block(b)
    entering = window[0]
    mark("pump4")
    pump("mixer")
    og_copy.wait()

    mark("mixer2")
    for b in range(NB):
        at = slice(b * BLOCK, (b + 1) * BLOCK)
        fade = jnp.concatenate(head_lanes(jnp.exp(blog[b : b + 1, 0:NH]), PER, 1), 1)
        state = before[b] + entering * fade
        high = state.astype(BF16)
        low = (state - high.astype(F32)).astype(BF16)
        read = rwc[at, 0:STATE]
        enter = matmul(read, high) + matmul(read, low)
        grown = jnp.concatenate(head_lanes(jnp.exp(cum_s[at, :]), PER, BLOCK), 1)
        gated = (inside[at, :] + enter * grown) * silu(og[at, :].astype(F32))
        scale = lax.rsqrt(jnp.mean(gated * gated, axis=-1, keepdims=True) + epsilon)
        normed[at, :] = (gated * scale * ggain[...]).astype(BF16)

    mark("outproj")
    NCH = 512
    i_p = [ids(), ids()]
    i_x = [ids(), ids()]
    HALF = SH // 2
    wout_copy.wait()
    mark("pump5")
    pump("project")
    mark("outproj")

    def rows_of(index):
        return pl.ds(pl.multiple_of(index * SH, SH), SH)

    for k, target in enumerate(((t_c + 2) % 4, t_c)):
        for n in range(0, D, NCH):
            psend[k, :, n : n + NCH] = matmul(
                normed[rows_of(target), :], wout[:, n : n + NCH]
            ).astype(BF16)
        send(psend.at[k], pgot.at[k], i_p[k], P_c)
    mark("outproj_c")
    recv(pgot.at[0], i_p[0])
    for h in range(2):
        rows = pl.ds(pl.multiple_of(t_x * SH + h * HALF, RIM), HALF)
        at = slice(h * HALF, (h + 1) * HALF)
        for n in range(0, D, NCH):
            xsend[at, n : n + NCH] = (
                matmul(normed[rows, :], wout[:, n : n + NCH])
                + pgot[0, at, n : n + NCH].astype(F32)
            ).astype(BF16)
        half = pl.ds(h * HALF, HALF)
        send(xsend.at[half, :], xgot.at[half, :], i_x[h], P_x)
    res_copy.wait()
    recv(pgot.at[1], i_p[1])
    for n in range(0, D, NCH):
        own_sum[:, n : n + NCH] = (
            matmul(normed[rows_of(t), :], wout[:, n : n + NCH])
            + pgot[1, :, n : n + NCH].astype(F32)
            + res[:, n : n + NCH].astype(F32)
        )
    RC = 16

    def rows_at(zi, ti, first=0, size=SH):
        return X.at[zi, pl.ds(pl.multiple_of(RIM + ti * SH + first, RIM), size), :]

    zo = 1 - zl
    i_a = [ids() for _ in range(14)]

    def half_at(zi, ti, h):
        return rows_at(zi, ti, h * HALF, HALF)

    def copy_to(i, device, *where):
        send(half_at(*where), half_at(*where), i_a[i], device)

    for h in range(2):
        mark(f"pump6{h}")
        pump(f"sum{h}")
        mark(f"xwait{h}")
        recv(xgot.at[pl.ds(h * HALF, HALF), :], i_x[h])
        for r in range(h * HALF, (h + 1) * HALF, RC):
            part_sum = own_sum[r : r + RC, :] + xgot[r : r + RC, :].astype(F32)
            kept = part_sum.astype(BF16)
            stream[r : r + RC, :] = kept
            floats = kept.astype(F32)
            scale = lax.rsqrt(jnp.mean(floats * floats, axis=-1, keepdims=True) + epsilon)
            X[zl, pl.ds(pl.multiple_of(RIM + t * SH + r, RC), RC), :] = (
                floats * scale * fgain[...]
            ).astype(BF16)
        copy_to(0 + h, P_x, zl, t, h)
        copy_to(2 + h, P_z, zl, t, h)
        copy_to(4 + h, P_c, zl, t, h)

    mark("gather")
    i_rim = [ids() for _ in range(2 * ntp)]
    nxt = s + 1
    nz, ny = nxt // 2, nxt % 2
    nzl = nz % 2
    rim_here = rows_at(zl, t, SH - RIM, RIM)
    for a in range(2):
        nz_to = nz if a == 0 else nz + 1 - 2 * nzl
        for ti in range(ntp):
            def go(nz_to=nz_to, ti=ti, j=a * ntp + ti):
                return pltpu.make_async_remote_copy(
                    src_ref=rim_here, dst_ref=X.at[nzl, pl.ds(0, RIM), :],
                    send_sem=ssem.at[i_rim[0] + j], recv_sem=rsem.at[i_rim[0] + nzl],
                    device_id=(2 * nz_to + ny, ti), device_id_type=MESH,
                )

            cond = (t == ntp - 1) & (nxt < nsp)
            pl.when(cond)(lambda go=go: go().start())
            pending.append(lambda go=go, cond=cond: pl.when(cond)(lambda: go().wait_send()))
    mark("pump8")
    pump("gather0")
    mark("gatherX0")
    recv(half_at(zo, t, 0), i_a[2])
    copy_to(6, P_x, zo, t, 0)
    copy_to(8, P_c, zo, t, 0)
    recv(half_at(zl, t_x, 0), i_a[0])
    copy_to(7, P_c, zl, t_x, 0)
    mark("pump9")
    pump("gather1")
    mark("gatherX1")
    recv(half_at(zo, t, 1), i_a[3])
    copy_to(9, P_x, zo, t, 1)
    copy_to(10, P_c, zo, t, 1)
    recv(half_at(zl, t_x, 1), i_a[1])
    copy_to(11, P_c, zl, t_x, 1)
    mark("pump10")
    pump("gather2")
    mark("gatherO")
    far_c = (t_c + 2) % 4
    recv(half_at(zl, t_c, 0), i_a[4])
    recv(half_at(zl, t_c, 1), i_a[5])
    recv(half_at(zl, far_c, 0), i_a[7])
    recv(half_at(zl, far_c, 1), i_a[11])
    for zi in range(2):
        first_block = 2 * (z - zl + zi) + y
        recv(X.at[zi, pl.ds(0, RIM), :], i_rim[0] + zi, first_block > 0)

        @pl.when(first_block == 0)
        def _(zi=zi):
            X[zi, 0:RIM, :] = jnp.zeros((RIM, D), BF16)

    mark("diagonal")
    recv(half_at(zo, t_x, 0), i_a[6])
    copy_to(12, P_c, zo, t_x, 0)
    recv(half_at(zo, t_x, 1), i_a[9])
    copy_to(13, P_c, zo, t_x, 1)

    def gather_rest():
        mark("gatherD")
        recv(half_at(zo, t_c, 0), i_a[8])
        recv(half_at(zo, t_c, 1), i_a[10])
        recv(half_at(zo, far_c, 0), i_a[12])
        recv(half_at(zo, far_c, 1), i_a[13])

    mark("ready01")
    pump("ready")
    ready(0)
    ready(1)
    pump("ffn")

    mark("ffn")
    MC = RIM + R // 2
    NC = 256
    KF = gtaps.shape[0]
    lane_f = lax.broadcasted_iota(jnp.int32, (KF, FS), 1)
    unused = outer & (lane_f >= FA)

    def my_taps(ref):
        taps = ref[...].astype(F32)
        taps = jnp.where(outer, taps[:, :FS], taps[:, FA:])
        return jnp.where(unused, 0.0, taps)

    gt, st = my_taps(gtaps), my_taps(staps)

    def one_half(zc, stop):

        def chunk(q, _):
            rows = pl.ds(pl.multiple_of(q * (R // 2), RIM), MC)
            for n in range(0, FS, NC):
                here = X[zc, rows, :]
                gs[rows, n : n + NC] = matmul(here, gfull[:, n : n + NC]).astype(BF16).astype(F32)
                vs[rows, n : n + NC] = matmul(here, vfull[:, n : n + NC]).astype(BF16).astype(F32)
            return 0

        lax.fori_loop(0, 2, chunk, 0)
        mark(stop)
        pump(stop)
        mark("conv_f")
        RB = 64
        for r in range(0, R, RB):
            for n in range(0, FS, NC):
                lanes = slice(n, n + NC)
                gate = jnp.zeros((RB, NC), F32)
                value = jnp.zeros((RB, NC), F32)
                for j in range(KF):
                    start = RIM - (KF - 1) + j + r
                    gate = gate + gt[j : j + 1, lanes] * gs[start : start + RB, lanes]
                    value = value + st[j : j + 1, lanes] * vs[start : start + RB, lanes]
                hidden[zc, r : r + RB, lanes] = (silu(gate) * value).astype(BF16)

    one_half(zl, "conv0")
    mark("pump11")
    pump("halves")
    gather_rest()
    mark("ffn2")
    one_half(zo, "conv1")

    HD = D // 4
    phase_ids = []

    def first_stage(p):
        mark(f"pump_down{p}")
        pump(f"down{p}")
        mark(f"ready2{p}")
        ready(2, p < 2, p % 2)
        half = (zh + p // 2) % 2
        i_o = [ids() for _ in range(4)]
        i_r = [ids() for _ in range(6)]
        phase_ids.append(i_r)
        order = ((zo, 1), (zl, 1), (zo, 0), (zl, 0))

        def down_rows(zi, ti, n, half=half, p=p):
            rows = pl.ds(pl.multiple_of(ti * SH, SH), SH)
            return matmul(hidden[zi, rows, :], dfull[half, p % 2, :, n : n + NCH])

        mark(f"down{p}")
        for k, (zi, far) in enumerate(order):
            ti = (t_c + 2 * far) % 4
            for n in range(0, HD, NCH):
                osend[p, k, :, n : n + NCH] = down_rows(zi, ti, n).astype(BF16)
            send(osend.at[p, k], cgot.at[p, k], i_o[k], P_c)
        mark(f"diag{p}")
        recv(cgot.at[p, 0], i_o[0])
        for n in range(0, HD, NCH):
            r2send[p, 2, :, n : n + NCH] = (
                down_rows(zo, t_x, n) + cgot[p, 0, :, n : n + NCH].astype(F32)
            ).astype(BF16)
        send(r2send.at[p, 2, pl.ds(0, HALF), :], r1got.at[p, pl.ds(0, HALF), :], i_r[0], P_x)
        send(r2send.at[p, 2, pl.ds(HALF, HALF), :], r1got.at[p, pl.ds(HALF, HALF), :], i_r[1], P_z)
        recv(cgot.at[p, 1], i_o[1])
        for n in range(0, HD, NCH):
            bx_sum[p % 2, :, n : n + NCH] = down_rows(zl, t_x, n) + cgot[p, 1, :, n : n + NCH].astype(F32)
        r2send[p, 0, 0:HALF, :] = bx_sum[p % 2, 0:HALF, :].astype(BF16)
        send(r2send.at[p, 0, pl.ds(0, HALF), :], r2got.at[p, 0, pl.ds(0, HALF), :], i_r[2], P_x)
        recv(cgot.at[p, 2], i_o[2])
        for n in range(0, HD, NCH):
            bz_sum[p % 2, :, n : n + NCH] = down_rows(zo, t, n) + cgot[p, 2, :, n : n + NCH].astype(F32)
        r2send[p, 1, HALF:, :] = bz_sum[p % 2, HALF:, :].astype(BF16)
        send(r2send.at[p, 1, pl.ds(HALF, HALF), :], r2got.at[p, 1, pl.ds(HALF, HALF), :], i_r[3], P_z)
        recv(cgot.at[p, 3], i_o[3])
        for n in range(0, HD, NCH):
            own_sum[:, p * HD + n : p * HD + n + NCH] = (
                down_rows(zl, t, n) + cgot[p, 3, :, n : n + NCH].astype(F32)
            )

    def second_stage(p):
        i_r = phase_ids[p]
        mark(f"r1wait{p}")
        first, second = pl.ds(0, HALF), pl.ds(HALF, HALF)
        recv(r1got.at[p, second, :], i_r[1])
        r2send[p, 0, HALF:, :] = (bx_sum[p % 2, HALF:, :] + r1got[p, HALF:, :].astype(F32)).astype(BF16)
        send(r2send.at[p, 0, second, :], r2got.at[p, 0, second, :], i_r[4], P_x)
        recv(r1got.at[p, first, :], i_r[0])
        r2send[p, 1, 0:HALF, :] = (bz_sum[p % 2, 0:HALF, :] + r1got[p, 0:HALF, :].astype(F32)).astype(BF16)
        send(r2send.at[p, 1, first, :], r2got.at[p, 1, first, :], i_r[5], P_z)

    first_stage(0)
    for p in range(1, 4):
        first_stage(p)
        second_stage(p - 1)
    second_stage(3)
    for p in range(4):
        i_r = phase_ids[p]
        half = (zh + p // 2) % 2
        mark(f"r2wait{p}")
        for h, (i_of_x, i_of_z) in enumerate(((i_r[2], i_r[5]), (i_r[4], i_r[3]))):
            recv(r2got.at[p, 0, pl.ds(h * HALF, HALF), :], i_of_x)
            recv(r2got.at[p, 1, pl.ds(h * HALF, HALF), :], i_of_z)
        mark(f"final{p}")
        for a in range(2):
            @pl.when(half == a)
            def _(a=a, p=p):
                for r in range(0, SH, RC):
                    here = slice(r, r + RC)
                    for j in range(HD // LANE):
                        from_ = slice(j * LANE, (j + 1) * LANE)
                        mine = slice(p * HD + j * LANE, p * HD + (j + 1) * LANE)
                        first = a * (D // 2) + j * KS + (p % 2) * LANE
                        cols = slice(first, first + LANE)
                        out[here, cols] = (
                            own_sum[here, mine]
                            + stream[here, cols].astype(F32)
                            + r2got[p, 0, here, from_].astype(F32)
                            + r2got[p, 1, here, from_].astype(F32)
                        ).astype(BF16)
    mark("drain")
    for f in pending:
        f()
    mark(None)
    assert counter[0] <= ssem.shape[0]
    assert len(moves) == NQ * (Z + 2)
    assert local_n[0] <= lsem.shape[0] - 4


def fused_dims(nsp, ntp, args):
    R, CH = args[0].shape
    NH = args[4].shape[1]
    D, F = args[12].shape[1], args[15].shape[1]
    fits = (
        nsp % 4 == 0 and nsp == 8 and ntp == 4
        and args[1].shape[1] == STATE and args[2].shape[1] == STATE
        and NH == 8 and CH == NH * HEAD and 2 * STATE == LANE
        and R % BLOCK == 0 and R % (ntp * 2 * RIM) == 0
        and D // nsp == 2 * LANE and D % 512 == 0 and F % LANE == 0
        and args[8].shape[0] <= 8 and args[17].shape[0] <= 8
    )
    FS = (F // LANE + 1) // 2 * LANE
    if not fits or FS % 256 or nsp % 8:
        return None
    return (R, CH, NH, D, F, FS, D // nsp, R // ntp)


def fused_on_device(nsp, ntp, dims, args):
    (
        xv, write, read, og, scores, extra, bias, rate, vtaps, wtaps, rtaps, ggain, wout, resid,
        fgain, gw, vw, gtaps, staps, dw,
    ) = args
    (R, CH, NH, D, F, FS, KS, SH) = dims
    Z, NB = nsp // 2, R // BLOCK
    rounds = max(1, (nsp - 2).bit_length())
    V = pltpu.VMEM
    msg_rows = STATE + 16
    scratch = [
        V((R, CH), BF16), V((R, CH), BF16), V((CH, D), BF16),
        V((RIM, CH), BF16), V((2, STATE, LANE), BF16), V((8 + R, CH), F32), V((8 + R, LANE), F32),
        V((R, CH), BF16), V((R, LANE), BF16), V((NB, LANE, BLOCK), BF16), V((2 * NH, R), F32),
        V((NH, R), F32), V((R, NH), F32), V((NB, STATE, CH), F32), V((NB + 2, LANE), F32),
        V((R, CH), F32), V((msg_rows, CH), BF16), V((STATE + 8, CH), F32),
        V((rounds, msg_rows, CH), BF16), V((rounds + 2, msg_rows, CH), BF16),
        V((R, CH), BF16), V((2, SH, D), BF16), V((2, SH, D), BF16),
        V((SH, D), BF16), V((SH, D), BF16), V((SH, D), F32), V((SH, D), BF16), V((SH, D), BF16),
        V((Z, KS, F), BF16), V((Z, KS, F), BF16), V((Z, F, KS), BF16),
        V((D, FS), BF16), V((D, FS), BF16), V((2, 2, FS, D // 4), BF16),
        V((2, RIM + R, D), BF16), V((RIM + R, FS), F32), V((RIM + R, FS), F32),
        V((2, R, FS), BF16), V((4, 4, SH, D // 4), BF16), V((4, 4, SH, D // 4), BF16),
        V((4, SH, D // 4), BF16), V((4, 3, SH, D // 4), BF16), V((4, 2, SH, D // 4), BF16),
        V((2, SH, D // 4), F32), V((2, SH, D // 4), F32),
        pltpu.SemaphoreType.DMA((288,)), pltpu.SemaphoreType.DMA((288,)),
        pltpu.SemaphoreType.DMA((80,)),
    ]
    vm, hbm = pl.BlockSpec(memory_space=pltpu.VMEM), pl.BlockSpec(memory_space=pl.ANY)
    return pl.pallas_call(
        functools.partial(fused_kernel, nsp, ntp, dims),
        out_shape=jax.ShapeDtypeStruct((SH, D), BF16),
        in_specs=[
            hbm, vm, vm, hbm, vm, vm, vm, vm, vm, vm, vm, vm, hbm, hbm, vm, hbm, hbm, vm, vm, hbm
        ],
        out_specs=vm,
        scratch_shapes=scratch,
        compiler_params=pltpu.CompilerParams(
            collective_id=0, has_side_effects=True, vmem_limit_bytes=67043328
        ),
    )(
        xv, write.T, read.T, og, scores.T, extra.T, bias.reshape(1, NH), rate.reshape(1, NH), vtaps,
        wtaps, rtaps, ggain.reshape(1, CH), wout, resid, fgain.reshape(1, D), gw, vw, gtaps, staps, dw,
    )


def on_device(nsp, ntp, *args):
    dims = fused_dims(nsp, ntp, args)
    if dims is None:
        return plain_on_device(*args)
    return fused_on_device(nsp, ntp, dims, args)


def solution(mesh):
    placed = (
        P("sp", "tp"),
        P("sp", "tp"),
        P("sp", "tp"),
        P("sp", "tp"),
        P("sp", "tp"),
        P("sp", "tp"),
        P("tp"),
        P("tp"),
        P(None, "tp"),
        P(None, "tp"),
        P(None, "tp"),
        P("tp"),
        P("tp", None),
        P("sp", None),
        P(),
        P("sp", "tp"),
        P("sp", "tp"),
        P(None, "tp"),
        P(None, "tp"),
        P("tp", "sp"),
    )
    return jax.shard_map(
        functools.partial(on_device, mesh.shape["sp"], mesh.shape["tp"]), mesh=mesh, in_specs=placed, out_specs=P(("sp", "tp"), None), check_vma=False
    )
```

```python
import functools

import jax
import jax.numpy as jnp
from jax import lax
from jax.experimental import pallas as pl
from jax.experimental.pallas import tpu as pltpu
from jax.sharding import PartitionSpec as P

HEAD = 64
STATE = 64
BLOCK = 128


epsilon = 1e-06


def from_behind(value, axis, by):
    length = lax.axis_size(axis)
    pairs = [(i, i + by) for i in range(length) if 0 <= i + by < length]
    return lax.ppermute(value, axis, pairs)


def entering_2(value, axis, join, neutral):
    count, mine = (lax.axis_size(axis), lax.axis_index(axis))

    def shifted(part, by):
        moved = from_behind(part, axis, by)
        return jnp.where(mine >= by, moved, neutral)

    if count == 1:
        return neutral
    window, width = (shifted(value, 1), 1)
    while width < count - 1:
        earlier = shifted(value, 2) if width == 1 else shifted(window, width)
        window, width = (join(earlier, window), 2 * width)
    return window


def halving_bits(axis):
    count = lax.axis_size(axis)
    return [1 << b for b in range(count.bit_length() - 1)] if count & (count - 1) == 0 else None


def swap(value, axis, bit):
    return lax.ppermute(value, axis, [(i, i ^ bit) for i in range(lax.axis_size(axis))])


def product_scattered(rows, weight, axis):
    count, mine = (lax.axis_size(axis), lax.axis_index(axis))
    bits = halving_bits(axis)
    if not bits:
        product = jnp.dot(rows, weight, preferred_element_type=jnp.float32)
        return lax.psum_scatter(product, axis, scatter_dimension=0, tiled=True)
    share = rows.shape[0] // count

    def side(array, which):
        return lax.dynamic_index_in_dim(
            array.reshape(array.shape[0] // 2, 2, *array.shape[1:]),
            which,
            1,
            keepdims=False,
            allow_negative_indices=False,
        )

    rows = rows.reshape(count, share, -1)

    def multiplied(part):
        flat = jnp.dot(
            part.reshape(-1, part.shape[-1]), weight, preferred_element_type=jnp.float32
        )
        return flat.reshape(part.shape[0], share, -1)

    low = mine & 1
    product = multiplied(rows)
    going = side(product, 1 - low).astype(jnp.bfloat16)
    arrived = swap(going, axis, 1)
    total = side(product, low)
    for bit in bits[1:]:
        own = (mine // bit) & 1
        going = (side(total, 1 - own) + side(arrived, 1 - own).astype(jnp.float32)).astype(
            jnp.bfloat16
        )
        total = side(total, own) + side(arrived, own).astype(jnp.float32)
        arrived = swap(going, axis, bit)
    return (total + arrived.astype(jnp.float32))[0]


def rows_gathered(own, axis):
    bits = halving_bits(axis)
    if not bits:
        return lax.all_gather(own, axis, axis=0, tiled=True)
    mine = lax.axis_index(axis)
    held = own[None]
    for bit in reversed(bits):
        other = swap(held, axis, bit)
        high = ((mine // bit) & 1) == 1
        held = jnp.stack([jnp.where(high, other, held), jnp.where(high, held, other)], 1)
        held = held.reshape(-1, *own.shape)
    return held.reshape(-1, own.shape[-1])


def put(whole, block, index):
    start = (index, *[jnp.zeros_like(index)] * block.ndim)
    return lax.dynamic_update_slice(whole, block[None], start, allow_negative_indices=False)


class RingGather:
    def __init__(self, block, axis):
        self.axis, self.count, self.step = (axis, lax.axis_size(axis), 0)
        count, mine = (self.count, lax.axis_index(axis))
        if count % 2:
            order = list(range(count))
            self.place = mine
        else:
            order = list(range(0, count, 2)) + list(range(count - 1, 0, -2))
            self.place = jnp.where(mine % 2 == 0, mine, 2 * count - 1 - mine) // 2
        self.forward = [(order[p], order[(p + 1) % count]) for p in range(count)]
        self.backward = [(b, a) for a, b in self.forward]
        self.up = self.down = block
        whole = jnp.zeros((count, *block.shape), block.dtype)
        self.whole = put(whole, block, mine)

    def owner(self, place):
        place = lax.rem(place + self.count, self.count)
        if self.count % 2:
            return place
        return jnp.where(2 * place < self.count, 2 * place, 2 * self.count - 1 - 2 * place)

    def advance(self):
        self.step += 1
        if self.step > self.count // 2:
            return
        self.up = lax.ppermute(self.up, self.axis, self.forward)
        self.whole = put(self.whole, self.up, self.owner(self.place - self.step))
        if self.step <= (self.count - 1) // 2:
            self.down = lax.ppermute(self.down, self.axis, self.backward)
            self.whole = put(self.whole, self.down, self.owner(self.place + self.step))

    def settle(self, value):
        value, self.up, self.down = lax.optimization_barrier((value, self.up, self.down))
        return value

    def gathered(self):
        while self.step < self.count // 2:
            self.advance()
        return self.whole.reshape(-1, self.whole.shape[-1])


def causal_taps(current, previous, kernel):
    tap_count = kernel.shape[0]
    length = current.shape[0]
    padded = jnp.concatenate([previous, current], 0).astype(jnp.float32)
    result = jnp.zeros((length, current.shape[1]), jnp.float32)
    for offset in range(tap_count):
        result = result + kernel[offset].astype(jnp.float32) * padded[offset : offset + length]
    return result


def channel_norm(stream, gain):
    floats = stream.astype(jnp.float32)
    scaled = floats * lax.rsqrt(jnp.mean(floats * floats, axis=-1, keepdims=True) + epsilon)
    return (scaled * gain).astype(jnp.bfloat16)


def plain_on_device(
    mixer_value_projection,
    write_vectors_projected,
    read_vectors_projected,
    output_gate_projected,
    step_size_scores,
    position_decay_extra,
    step_size_bias,
    head_decay_logarithm,
    value_filter_taps,
    write_filter_taps,
    read_filter_taps,
    gated_group_norm_gain,
    mixer_output_weight,
    residual,
    feedforward_norm_gain,
    feedforward_gate_weight,
    feedforward_value_weight,
    gate_filter_taps,
    single_value_filter_taps,
    feedforward_down_weight,
):
    row_count = mixer_value_projection.shape[0]
    head_count = step_size_scores.shape[1]
    group_count = write_vectors_projected.shape[1] // STATE
    per_group = head_count // group_count
    mix_rim = value_filter_taps.shape[0] - 1
    channels = (mixer_value_projection.shape[1], write_vectors_projected.shape[1])
    rims = from_behind(
        jnp.concatenate(
            [
                mixer_value_projection[row_count - mix_rim :],
                write_vectors_projected[row_count - mix_rim :],
                read_vectors_projected[row_count - mix_rim :],
            ],
            1,
        ),
        "sp",
        1,
    )
    rim_values, rim_write, rim_read = jnp.split(rims, [channels[0], sum(channels)], axis=1)
    by_ring = feedforward_gate_weight.shape[1] // 256 * 128
    gate_ring = RingGather(feedforward_gate_weight[:, :by_ring], "sp")
    gate_ring.advance()
    x_conv = jax.nn.silu(causal_taps(mixer_value_projection, rim_values, value_filter_taps)).astype(
        jnp.bfloat16
    )
    write_conv = jax.nn.silu(
        causal_taps(write_vectors_projected, rim_write, write_filter_taps)
    ).astype(jnp.bfloat16)
    read_conv = jax.nn.silu(causal_taps(read_vectors_projected, rim_read, read_filter_taps)).astype(
        jnp.bfloat16
    )
    step_size_head = jax.nn.softplus(step_size_scores + step_size_bias)
    logarithm_decay_rate = -step_size_head * jnp.exp(head_decay_logarithm) + position_decay_extra
    scaled = (
        x_conv.astype(jnp.float32).reshape(row_count, head_count, HEAD) * step_size_head[:, :, None]
    ).astype(jnp.bfloat16)
    block_count = row_count // BLOCK
    value_blocks = scaled.reshape(block_count, BLOCK, group_count, per_group, HEAD)
    write_blocks = write_conv.reshape(block_count, BLOCK, group_count, STATE)
    read_blocks = read_conv.reshape(block_count, BLOCK, group_count, STATE)
    running = jnp.cumsum(logarithm_decay_rate.reshape(block_count, BLOCK, head_count), axis=1)
    by_head = jnp.moveaxis(running, 1, 2)
    spread = by_head[..., :, None] - by_head[..., None, :]
    causal = jnp.tril(jnp.ones((BLOCK, BLOCK), dtype=jnp.bool_))
    decays = jnp.exp(jnp.where(causal, spread, -jnp.inf)).reshape(
        block_count, group_count, per_group, BLOCK, BLOCK
    )
    scores = jnp.einsum(
        "blgn,bsgn->bgls", read_blocks, write_blocks, preferred_element_type=jnp.float32
    )
    weights = (scores[:, :, None] * decays).astype(jnp.bfloat16)
    inside = jnp.einsum(
        "bgrls,bsgrp->blgrp", weights, value_blocks, preferred_element_type=jnp.float32
    )
    tails = jnp.moveaxis(jnp.exp(by_head[..., -1:] - by_head), 2, 1).reshape(
        block_count, BLOCK, group_count, per_group
    )
    tailed = (value_blocks.astype(jnp.float32) * tails[..., None]).astype(jnp.bfloat16)
    fresh = jnp.einsum(
        "bsgn,bsgrp->bgrnp", write_blocks, tailed, preferred_element_type=jnp.float32
    )
    fresh = gate_ring.settle(fresh)
    gate_ring.advance()
    block_logs = by_head[..., -1].reshape(block_count, group_count, per_group)

    empty_state = jnp.zeros((group_count, per_group, STATE, HEAD), jnp.float32)
    block_decays = jnp.exp(block_logs)
    before, carried = ([], empty_state)
    for block in range(block_count):
        before.append(carried)
        carried = carried * block_decays[block][..., None, None] + fresh[block]
    local_before, local_end = (jnp.stack(before), carried)
    device_decay = jnp.exp(jnp.sum(block_logs, axis=0))

    def packed(decay, state):
        row = jnp.broadcast_to(decay[..., None, None], (*decay.shape, 8, HEAD))
        return jnp.concatenate([state, row], 2)

    def combine(earlier, later):
        decay = later[:, :, STATE : STATE + 1]
        state = earlier[:, :, :STATE] * decay + later[:, :, :STATE]
        return jnp.concatenate([state, earlier[:, :, STATE:] * decay], 2)

    identity = packed(jnp.ones((group_count, per_group), jnp.float32), empty_state)
    incoming = entering_2(packed(device_decay, local_end), "sp", combine, identity)[:, :, :STATE]
    incoming = gate_ring.settle(incoming)
    gate_ring.advance()
    before_block = jnp.cumsum(block_logs, axis=0) - block_logs
    entering_state = local_before + incoming[None] * jnp.exp(before_block)[..., None, None]
    entering = jnp.einsum(
        "blgn,bgrnp->blgrp",
        read_blocks.astype(jnp.float32),
        entering_state,
        precision=lax.Precision.HIGHEST,
    )
    entering = (
        entering * jnp.exp(running).reshape(block_count, BLOCK, group_count, per_group)[..., None]
    )
    mixer = (inside + entering).reshape(row_count, head_count * HEAD)
    gated = (mixer * jax.nn.silu(output_gate_projected.astype(jnp.float32))).reshape(
        row_count, group_count, -1
    )
    gated = gated * lax.rsqrt(jnp.mean(gated * gated, axis=-1, keepdims=True) + epsilon)
    normed = (gated.reshape(row_count, -1) * gated_group_norm_gain).astype(jnp.bfloat16)
    share = row_count // lax.axis_size("tp")
    tp_index = lax.axis_index("tp")
    normed = gate_ring.settle(normed)
    gate_ring.advance()
    summed = product_scattered(normed, mixer_output_weight, "tp")
    own_residual = lax.dynamic_slice_in_dim(residual, tp_index * share, share, 0)
    stream = (own_residual.astype(jnp.float32) + summed).astype(jnp.bfloat16)
    ffn_rows = rows_gathered(channel_norm(stream, feedforward_norm_gain), "tp")
    gate_rest = lax.all_gather(feedforward_gate_weight[:, by_ring:], "sp", axis=0, tiled=True)
    value_full = lax.all_gather(feedforward_value_weight, "sp", axis=0, tiled=True)
    gate_full = jnp.concatenate([gate_ring.gathered(), gate_rest], 1)
    gate_sum = jnp.dot(ffn_rows, gate_full, preferred_element_type=jnp.float32)
    value_sum = jnp.dot(ffn_rows, value_full, preferred_element_type=jnp.float32)
    gate_rows = gate_sum.astype(jnp.bfloat16)
    value_rows = value_sum.astype(jnp.bfloat16)
    ffn_rim = gate_filter_taps.shape[0] - 1
    rim_gate, rim_value = from_behind(
        (gate_rows[row_count - ffn_rim :], value_rows[row_count - ffn_rim :]), "sp", 1
    )
    hidden = (
        jax.nn.silu(causal_taps(gate_rows, rim_gate, gate_filter_taps))
        * causal_taps(value_rows, rim_value, single_value_filter_taps)
    ).astype(jnp.bfloat16)
    down_full = lax.all_gather(feedforward_down_weight, "sp", axis=1, tiled=True)
    down = product_scattered(hidden, down_full, "tp")
    return (stream.astype(jnp.float32) + down).astype(jnp.bfloat16)


MESH = pl.DeviceIdType.MESH
LANE = 128
RIM = 16
PLAN = {
    "start": ("B0", "B1", "E0", "E1", "E2", "Y0", "Y1", "Y2",),
    "scan1": ("B2", "E3",),
    "scan2": ("Y3", "E4",),
    "scan3": ("B3", "Y4", "E5", "Y5", "E6",),
    "mixer": ("S01", "B4", "Y6", "E7",),
    "project": ("S11", "B5", "Y7",),
    "sum0": ("S21", "B6", "S02", "S31",),
    "sum1": ("S12", "S41", "B7", "S03",),
    "gather0": ("S51", "S22", "S61", "S32", "S13",),
    "gather1": ("S71", "B8", "S42", "S23",),
    "gather2": ("S52", "S33", "S62", "B9", "S43", "S72", "E8", "S53", "S63", "E9", "S73", "Y8", "Y9",),
    "ffn": ("S81",),
    "conv0": ("S91",),
    "conv1": ("S82",),
    "down0": (),
    "down1": ("S92", "S83",),
    "down2": ("S93",),
    "down3": (),
}
F32, BF16 = jnp.float32, jnp.bfloat16


def matmul(a, b):
    return jnp.dot(a, b, preferred_element_type=F32)


def silu(v):
    half = 0.5 * v
    return half + half * jnp.tanh(half)


def head_lanes(columns, per_tile, rows):
    lane = lax.broadcasted_iota(jnp.int32, (rows, LANE), 1)
    tiles = []
    for first in range(0, columns.shape[1], per_tile):
        tile = jnp.broadcast_to(columns[:, first : first + 1], (rows, LANE))
        for k in range(1, per_tile):
            other = jnp.broadcast_to(columns[:, first + k : first + k + 1], (rows, LANE))
            tile = jnp.where(lane < k * HEAD, tile, other)
        tiles.append(tile)
    return tiles


def fused_kernel(nsp, ntp, dims, *refs):
    (R, CH, NH, D, F, FS, KS, SH) = dims
    (
        xv, wT, rT, og_in, scT, exT, bias, rate, vtaps, wtaps, rtaps, ggain, wout_in, resid, fgain,
        gw, vw, gtaps, staps, dw,
        out,
        og, wout, halo_x, halo_rw, rwf, rwc, rwT, steps, cumT_s, cum_s, before, blog,
        msg, winf, win, got,
        normed, psend, pgot, xsend, xgot, own_sum, res, stream,
        gst, vst, dst, gfull, vfull, dfull, X, gs, vs, hidden, osend, cgot, r1got, r2send, r2got,
        bx_sum, bz_sum,
        ssem, rsem, lsem,
    ) = refs
    xin = scaled = normed
    xf = vs.at[0, pl.ds(0, 8 + R), pl.ds(0, CH)]
    inside = gs.at[0, pl.ds(0, R), pl.ds(0, CH)]
    Z = nsp // 2
    NB = R // BLOCK
    NT = CH // LANE
    PER = LANE // HEAD
    FA = F - FS
    s, t = lax.axis_index("sp"), lax.axis_index("tp")
    z, y = s // 2, s % 2
    zl, zh = z % 2, z // 2
    x, c = t // 2, t % 2
    outer = (z % 4) * (3 - z % 4) == 0
    inner = jnp.logical_not(outer)
    s_z = s + 2 - 4 * zl
    s_y = s + 1 - 2 * y
    t_c = t + 1 - 2 * c
    t_x = (t + 2) % 4
    P_c, P_x, P_z, P_y = (s, t_c), (s, t_x), (s_z, t), (s_y, t)

    barrier = pltpu.get_barrier_semaphore()
    for i in range(nsp):
        for j in range(ntp):
            @pl.when((s != i) | (t != j))
            def _(i=i, j=j):
                pl.semaphore_signal(barrier, inc=1, device_id=(i, j), device_id_type=MESH)

    pl.semaphore_wait(barrier, nsp * ntp - 1)
    counter = [0]
    pending = []
    scope = [None]

    def mark(name):
        if scope[0] is not None:
            scope[0].__exit__(None, None, None)
        scope[0] = jax.named_scope(name) if name else None
        if name:
            scope[0].__enter__()

    def ids(n=1):
        first = counter[0]
        counter[0] += n
        return first

    def rcopy(src, dest, i, device):
        return pltpu.make_async_remote_copy(
            src_ref=src, dst_ref=dest, send_sem=ssem.at[i], recv_sem=rsem.at[i],
            device_id=device, device_id_type=MESH,
        )

    def send(src, dest, i, device, cond=None):
        def go():
            rcopy(src, dest, i, device).start()

        def done():
            rcopy(src, dest, i, device).wait_send()

        if cond is None:
            go()
            pending.append(done)
        else:
            pl.when(cond)(go)
            pending.append(lambda: pl.when(cond)(done))

    def recv(dest, i, cond=None):
        def go():
            rcopy(dest, dest, i, P_c).wait_recv()

        if cond is None:
            go()
        else:
            pl.when(cond)(go)

    own_w, stage, full = (gw, vw, dw), (gst, vst, dst), (gfull, vfull, dfull)
    cuts = [(m, h, (4, 4, 2)[m]) for m in range(3) for h in range((4, 4, 2)[m])]
    NQ = len(cuts)
    hop_id = [[[ids() for _ in range(Z)] for _ in range(2)] for _ in cuts]
    y_id = [[ids() for _ in range(2 * Z)] for _ in cuts]
    local_n = [0]
    landed = [[] for _ in range(3)]

    def part(q, ref, start, size):
        m, h, n = cuts[q]
        step_q = KS // n
        if m < 2:
            return ref.at[pl.ds(h * step_q, step_q), pl.ds(start, size)]
        return ref.at[pl.ds(start, size), pl.ds(h * step_q, step_q)]

    def place(q, shard):
        m, h, n = cuts[q]
        step_q = KS // n
        if m < 2:
            first = (2 * (shard % 2) + y) * KS + h * step_q
            return full[m].at[shard // 2, pl.ds(pl.multiple_of(first, step_q), step_q), :]
        near = (2 * (shard % 2) + y) * step_q
        return full[m].at[shard // 2, h, :, pl.ds(pl.multiple_of(near, step_q), step_q)]

    def forward(q, k, inward=True, outward=True):
        m = cuts[q][0]
        for up in (True, False):
            shard = z - (k - 1) if up else z + (k - 1)
            to = s + 2 if up else s - 2
            src = own_w[m] if k == 1 else stage[m].at[shard]
            dest = stage[m].at[shard]
            i = hop_id[q][0 if up else 1][k]
            have = (z >= k - 1) if up else (z <= Z - k)
            if up:
                long, short = have & (z < Z - 2), have & (z == Z - 2)
            else:
                long, short = have & (z > 1), have & (z == 1)
            if inward:
                send(part(q, src, 0, F), part(q, dest, 0, F), i, (to, t), long)
            if outward:
                send(part(q, src, 0, FA), part(q, dest, 0, FA), i, (to, t), short)

    def head_of(q, ref, size):
        if cuts[q][0] < 2:
            return ref.at[:, pl.ds(0, size)]
        return ref.at[pl.ds(0, size), :]

    def both(a, b):
        return a if b is None else (b if a is None else a & b)

    def deliver(q, shard, src, slot, cond, group):
        m = cuts[q][0]
        target = place(q, shard)
        i = y_id[q][slot]
        n = local_n[0]
        local_n[0] += 1
        kinds = []
        for kind, start, size in ((outer, 0, FA), (inner, FA, FS)):
            when = both(cond, kind)
            piece, landing = part(q, src, start, size), head_of(q, target, size)
            send(piece, landing, i, P_y, when)
            local = pltpu.make_async_copy(piece, landing, lsem.at[n])
            pl.when(when)(lambda local=local: local.start())
            kinds.append((when, local, landing))

        def wait(extra=None):
            for when, local, landing in kinds:
                def go(local=local, landing=landing):
                    local.wait()
                    rcopy(landing, landing, i, P_c).wait_recv()

                pl.when(both(when, extra))(go)

        landed[m].append((wait, group, cuts[q][1]))

    def service(q, k):
        m = cuts[q][0]
        for up in (True, False):
            i = hop_id[q][0 if up else 1][k]
            shard = z - k if up else z + k
            have = (z >= k) if up else (z <= Z - 1 - k)
            edge = (z == Z - 1) if up else (z == 0)
            dest = stage[m].at[shard]
            recv(part(q, dest, 0, F), i, have & jnp.logical_not(edge))
            recv(part(q, dest, 0, FA), i, have & edge)
        if k + 1 < Z:
            forward(q, k + 1)
        for up in (True, False):
            shard = z - k if up else z + k
            have = (z >= k) if up else (z <= Z - 1 - k)
            near = (shard // 2) == zh
            deliver(q, shard, stage[m].at[shard], k if up else Z - 1 + k, have, near)

    def ready(m, near=None, piece=None):
        for wait, group, h in landed[m]:
            if near is None:
                wait()
            elif piece is None or h == piece:
                if group is not None:
                    wait(group if near else jnp.logical_not(group))
                elif near:
                    wait()

    moves = []

    def pump(stop):
        for move in PLAN[stop]:
            assert move not in moves
            moves.append(move)
            q = int(move[1])
            if move[0] == "B":
                forward(q, 1, outward=False)
            elif move[0] == "E":
                forward(q, 1, inward=False)
            elif move[0] == "Y":
                deliver(q, z, own_w[cuts[q][0]], 0, None, None)
            else:
                service(q, int(move[2]))

    mark("rims")
    i_hx, i_hr = ids(), [ids(), ids()]
    send(xv.at[pl.ds(R - RIM, RIM), :], halo_x, i_hx, (s + 1, t), s < nsp - 1)
    send(rT.at[:, pl.ds(R - LANE, LANE)], halo_rw.at[0], i_hr[0], (s + 1, t), s < nsp - 1)
    send(wT.at[:, pl.ds(R - LANE, LANE)], halo_rw.at[1], i_hr[1], (s + 1, t), s < nsp - 1)
    NL = lsem.shape[0]
    x_copy = pltpu.make_async_copy(xv, xin, lsem.at[NL - 1])
    og_copy = pltpu.make_async_copy(og_in, og, lsem.at[NL - 2])
    wout_copy = pltpu.make_async_copy(wout_in, wout, lsem.at[NL - 3])
    res_copy = pltpu.make_async_copy(
        resid.at[pl.ds(pl.multiple_of(t * SH, SH), SH), :], res, lsem.at[NL - 4]
    )
    x_copy.start()
    pump("start")
    og_copy.start()
    wout_copy.start()
    res_copy.start()

    @pl.when(outer)
    def _():
        gfull[:, :, FA:] = jnp.zeros((2, D // 2, FS - FA), BF16)
        vfull[:, :, FA:] = jnp.zeros((2, D // 2, FS - FA), BF16)
        dfull[:, :, FA:, :] = jnp.zeros((2, 2, FS - FA, D // 4), BF16)

    @pl.when(s == 0)
    def _():
        halo_x[...] = jnp.zeros_like(halo_x)
        halo_rw[...] = jnp.zeros_like(halo_rw)

    eye = lax.broadcasted_iota(jnp.int32, (NH, NH), 0) == lax.broadcasted_iota(jnp.int32, (NH, NH), 1)

    def column(ref):
        return jnp.sum(jnp.where(eye, jnp.broadcast_to(ref[...], (NH, NH)), 0.0), 1, keepdims=True)

    raw = scT[...] + column(bias)
    soft = jnp.maximum(raw, 0.0) + jnp.log1p(jnp.exp(-jnp.abs(raw)))
    steps[0:NH, :] = soft
    steps[NH : 2 * NH, :] = exT[...] - soft * jnp.exp(column(rate))

    def pair(first, second):
        return jnp.concatenate([first.astype(F32), second.astype(F32)], 0).T

    for b in range(NB):
        at = slice(b * BLOCK, (b + 1) * BLOCK)
        rwf[8 + b * BLOCK : 8 + (b + 1) * BLOCK, :] = pair(rT[:, at], wT[:, at])
    x_copy.wait()
    xf[8:, :] = xin[...].astype(F32)
    recv(halo_x, i_hx, s > 0)
    recv(halo_rw.at[0], i_hr[0], s > 0)
    recv(halo_rw.at[1], i_hr[1], s > 0)
    xf[:8, :] = halo_x[...].astype(F32)[RIM - 8 :]
    rwf[:8, :] = pair(halo_rw[0], halo_rw[1])[LANE - 8 :]

    mark("convs")
    vt = vtaps[...].astype(F32)
    rt = jnp.concatenate([rtaps[...].astype(F32), wtaps[...].astype(F32)], 1)
    K = vt.shape[0]
    row = lax.broadcasted_iota(jnp.int32, (BLOCK, BLOCK), 0)
    col = lax.broadcasted_iota(jnp.int32, (BLOCK, BLOCK), 1)
    upper = (row <= col).astype(F32)
    carried = jnp.zeros((STATE, CH), F32)
    total = jnp.zeros((1, NH), F32)
    for b in range(NB):
        at = slice(b * BLOCK, (b + 1) * BLOCK)
        step_t = steps[0:NH, at]
        cum_t = jnp.dot(
            steps[NH : 2 * NH, at], upper, preferred_element_type=F32,
            precision=lax.Precision.HIGHEST,
        )
        step, cum = step_t.T, cum_t.T
        cumT_s[:, at] = cum_t
        cum_s[at, :] = cum
        last = cum[BLOCK - 1 : BLOCK, :]
        tails = head_lanes(jnp.exp(last - cum), PER, BLOCK)
        step_tiles = head_lanes(step, PER, BLOCK)
        rw_conv = jnp.zeros((BLOCK, rwf.shape[1]), F32)
        for j in range(K):
            start = 8 - (K - 1) + j + b * BLOCK
            rw_conv = rw_conv + rt[j : j + 1, :] * rwf[start : start + BLOCK, :]
        rw_conv = silu(rw_conv)
        rwc[at, :] = rw_conv.astype(BF16)
        turned = rw_conv.T.astype(BF16)
        rwT[b] = turned
        parts = []
        for p in range(NT):
            lanes = slice(p * LANE, (p + 1) * LANE)
            conv = jnp.zeros((BLOCK, LANE), F32)
            for j in range(K):
                start = 8 - (K - 1) + j + b * BLOCK
                conv = conv + vt[j : j + 1, lanes] * xf[start : start + BLOCK, lanes]
            conv = silu(conv).astype(BF16).astype(F32)
            value = (conv * step_tiles[p]).astype(BF16)
            scaled[at, lanes] = value
            parts.append((value.astype(F32) * tails[p]).astype(BF16))
        fresh = matmul(turned[STATE:], jnp.concatenate(parts, 1))
        before[b] = carried
        blog[b : b + 1, 0:NH] = total
        decay = jnp.concatenate(head_lanes(jnp.exp(last), PER, 1), 1)
        carried = carried * decay + fresh
        total = total + last

    def pack(ref, state, decay):
        ref[0:STATE, :] = state.astype(BF16)
        high = decay.astype(BF16)
        ref[STATE : STATE + 8, :] = jnp.broadcast_to(high, (8, CH))
        ref[STATE + 8 :, :] = jnp.broadcast_to((decay - high.astype(F32)).astype(BF16), (8, CH))

    pack(msg, carried, jnp.concatenate(head_lanes(jnp.exp(total), PER, 1), 1))

    mark("scan")

    def shift(source, slot, i, by):
        send(source, got.at[slot], i, (s + by, t), s + by < nsp)

    def arrived(slot, i, by):
        recv(got.at[slot], i, s >= by)

        @pl.when(s < by)
        def _():
            got[slot, 0:STATE, :] = jnp.zeros((STATE, CH), BF16)
            got[slot, STATE : STATE + 8, :] = jnp.ones((8, CH), BF16)
            got[slot, STATE + 8 :, :] = jnp.zeros((8, CH), BF16)

    def unpack(ref):
        tail = ref[STATE:, :].astype(F32)
        return ref[0:STATE, :].astype(F32), tail[0:1] + tail[8:9]

    def join(earlier, later):
        return earlier[0] * later[1] + later[0], earlier[1] * later[1]

    widths = []
    width = 1
    while width < nsp - 1:
        widths.append(2 if width == 1 else width)
        width *= 2
    scan_ids = [ids() for _ in range(len(widths) + 1)]
    shift(msg, 0, scan_ids[0], 1)
    shift(msg, 1, scan_ids[1], 2)
    pump("scan1")

    causal = row >= col
    lane_b = lax.broadcasted_iota(jnp.int32, (BLOCK, LANE), 1)

    def inside_block(b):
        at = slice(b * BLOCK, (b + 1) * BLOCK)
        scores = matmul(rwc[at, 0:STATE], rwT[b, STATE:, :])
        cum, cum_t = cum_s[at, :], cumT_s[:, at]
        for p in range(NT):
            lanes = slice(p * LANE, (p + 1) * LANE)
            value = scaled[at, lanes].astype(F32)
            left, right = [], []
            for k in range(PER):
                h = p * PER + k
                spread = cum[:, h : h + 1] - cum_t[h : h + 1, :]
                left.append((scores * jnp.exp(jnp.where(causal, spread, -jnp.inf))).astype(BF16))
                mine = (lane_b >= k * HEAD) & (lane_b < (k + 1) * HEAD)
                right.append(jnp.where(mine, value, 0.0).astype(BF16))
            inside[at, lanes] = matmul(jnp.concatenate(left, 1), jnp.concatenate(right, 0))

    third = (NB + 2) // 3
    for b in range(0, third):
        inside_block(b)
    mark("scan1")
    arrived(0, scan_ids[0], 1)
    arrived(1, scan_ids[1], 2)
    window = join(unpack(got.at[1]), unpack(got.at[0]))
    done_blocks = third
    for r, by in enumerate(widths[1:]):
        pack(win.at[r], *window)
        winf[0:STATE, :] = window[0]
        winf[STATE:, :] = jnp.broadcast_to(window[1], (8, CH))
        shift(win.at[r], r + 2, scan_ids[r + 2], by)
        pump(f"scan{r + 2}")
        for b in range(done_blocks, min(NB, done_blocks + third)):
            inside_block(b)
        done_blocks = min(NB, done_blocks + third)
        mark(f"scan{r + 2}")
        arrived(r + 2, scan_ids[r + 2], by)
        window = join(unpack(got.at[r + 2]), (winf[0:STATE, :], winf[STATE : STATE + 1, :]))
    for b in range(done_blocks, NB):
        inside_block(b)
    entering = window[0]
    mark("pump4")
    pump("mixer")
    og_copy.wait()

    mark("mixer2")
    for b in range(NB):
        at = slice(b * BLOCK, (b + 1) * BLOCK)
        fade = jnp.concatenate(head_lanes(jnp.exp(blog[b : b + 1, 0:NH]), PER, 1), 1)
        state = before[b] + entering * fade
        high = state.astype(BF16)
        low = (state - high.astype(F32)).astype(BF16)
        read = rwc[at, 0:STATE]
        enter = matmul(read, high) + matmul(read, low)
        grown = jnp.concatenate(head_lanes(jnp.exp(cum_s[at, :]), PER, BLOCK), 1)
        gated = (inside[at, :] + enter * grown) * silu(og[at, :].astype(F32))
        scale = lax.rsqrt(jnp.mean(gated * gated, axis=-1, keepdims=True) + epsilon)
        normed[at, :] = (gated * scale * ggain[...]).astype(BF16)

    mark("outproj")
    NCH = 512
    i_p = [ids(), ids()]
    i_x = [ids(), ids()]
    HALF = SH // 2
    wout_copy.wait()
    mark("pump5")
    pump("project")
    mark("outproj")

    def rows_of(index):
        return pl.ds(pl.multiple_of(index * SH, SH), SH)

    for k, target in enumerate(((t_c + 2) % 4, t_c)):
        for n in range(0, D, NCH):
            psend[k, :, n : n + NCH] = matmul(
                normed[rows_of(target), :], wout[:, n : n + NCH]
            ).astype(BF16)
        send(psend.at[k], pgot.at[k], i_p[k], P_c)
    mark("outproj_c")
    recv(pgot.at[0], i_p[0])
    for h in range(2):
        rows = pl.ds(pl.multiple_of(t_x * SH + h * HALF, RIM), HALF)
        at = slice(h * HALF, (h + 1) * HALF)
        for n in range(0, D, NCH):
            xsend[at, n : n + NCH] = (
                matmul(normed[rows, :], wout[:, n : n + NCH])
                + pgot[0, at, n : n + NCH].astype(F32)
            ).astype(BF16)
        half = pl.ds(h * HALF, HALF)
        send(xsend.at[half, :], xgot.at[half, :], i_x[h], P_x)
    res_copy.wait()
    recv(pgot.at[1], i_p[1])
    for n in range(0, D, NCH):
        own_sum[:, n : n + NCH] = (
            matmul(normed[rows_of(t), :], wout[:, n : n + NCH])
            + pgot[1, :, n : n + NCH].astype(F32)
            + res[:, n : n + NCH].astype(F32)
        )
    RC = 16

    def rows_at(zi, ti, first=0, size=SH):
        return X.at[zi, pl.ds(pl.multiple_of(RIM + ti * SH + first, RIM), size), :]

    zo = 1 - zl
    i_a = [ids() for _ in range(14)]

    def half_at(zi, ti, h):
        return rows_at(zi, ti, h * HALF, HALF)

    def copy_to(i, device, *where):
        send(half_at(*where), half_at(*where), i_a[i], device)

    for h in range(2):
        mark(f"pump6{h}")
        pump(f"sum{h}")
        mark(f"xwait{h}")
        recv(xgot.at[pl.ds(h * HALF, HALF), :], i_x[h])
        for r in range(h * HALF, (h + 1) * HALF, RC):
            part_sum = own_sum[r : r + RC, :] + xgot[r : r + RC, :].astype(F32)
            kept = part_sum.astype(BF16)
            stream[r : r + RC, :] = kept
            floats = kept.astype(F32)
            scale = lax.rsqrt(jnp.mean(floats * floats, axis=-1, keepdims=True) + epsilon)
            X[zl, pl.ds(pl.multiple_of(RIM + t * SH + r, RC), RC), :] = (
                floats * scale * fgain[...]
            ).astype(BF16)
        copy_to(0 + h, P_x, zl, t, h)
        copy_to(2 + h, P_z, zl, t, h)
        copy_to(4 + h, P_c, zl, t, h)

    mark("gather")
    i_rim = [ids() for _ in range(2 * ntp)]
    nxt = s + 1
    nz, ny = nxt // 2, nxt % 2
    nzl = nz % 2
    rim_here = rows_at(zl, t, SH - RIM, RIM)
    for a in range(2):
        nz_to = nz if a == 0 else nz + 1 - 2 * nzl
        for ti in range(ntp):
            def go(nz_to=nz_to, ti=ti, j=a * ntp + ti):
                return pltpu.make_async_remote_copy(
                    src_ref=rim_here, dst_ref=X.at[nzl, pl.ds(0, RIM), :],
                    send_sem=ssem.at[i_rim[0] + j], recv_sem=rsem.at[i_rim[0] + nzl],
                    device_id=(2 * nz_to + ny, ti), device_id_type=MESH,
                )

            cond = (t == ntp - 1) & (nxt < nsp)
            pl.when(cond)(lambda go=go: go().start())
            pending.append(lambda go=go, cond=cond: pl.when(cond)(lambda: go().wait_send()))
    mark("pump8")
    pump("gather0")
    mark("gatherX0")
    recv(half_at(zo, t, 0), i_a[2])
    copy_to(6, P_x, zo, t, 0)
    copy_to(8, P_c, zo, t, 0)
    recv(half_at(zl, t_x, 0), i_a[0])
    copy_to(7, P_c, zl, t_x, 0)
    mark("pump9")
    pump("gather1")
    mark("gatherX1")
    recv(half_at(zo, t, 1), i_a[3])
    copy_to(9, P_x, zo, t, 1)
    copy_to(10, P_c, zo, t, 1)
    recv(half_at(zl, t_x, 1), i_a[1])
    copy_to(11, P_c, zl, t_x, 1)
    mark("pump10")
    pump("gather2")
    mark("gatherO")
    far_c = (t_c + 2) % 4
    recv(half_at(zl, t_c, 0), i_a[4])
    recv(half_at(zl, t_c, 1), i_a[5])
    recv(half_at(zl, far_c, 0), i_a[7])
    recv(half_at(zl, far_c, 1), i_a[11])
    for zi in range(2):
        first_block = 2 * (z - zl + zi) + y
        recv(X.at[zi, pl.ds(0, RIM), :], i_rim[0] + zi, first_block > 0)

        @pl.when(first_block == 0)
        def _(zi=zi):
            X[zi, 0:RIM, :] = jnp.zeros((RIM, D), BF16)

    mark("diagonal")
    recv(half_at(zo, t_x, 0), i_a[6])
    copy_to(12, P_c, zo, t_x, 0)
    recv(half_at(zo, t_x, 1), i_a[9])
    copy_to(13, P_c, zo, t_x, 1)

    def gather_rest():
        mark("gatherD")
        recv(half_at(zo, t_c, 0), i_a[8])
        recv(half_at(zo, t_c, 1), i_a[10])
        recv(half_at(zo, far_c, 0), i_a[12])
        recv(half_at(zo, far_c, 1), i_a[13])

    mark("ffn")
    MC = RIM + R // 2
    NC = 256
    KF = gtaps.shape[0]
    lane_f = lax.broadcasted_iota(jnp.int32, (KF, FS), 1)
    unused = outer & (lane_f >= FA)

    def my_taps(ref):
        taps = ref[...].astype(F32)
        taps = jnp.where(outer, taps[:, :FS], taps[:, FA:])
        return jnp.where(unused, 0.0, taps)

    gt, st = my_taps(gtaps), my_taps(staps)

    def products(zc, far):
        half = (zh + far) % 2
        lanes_in = pl.ds(pl.multiple_of(half * (D // 2), D // 2), D // 2)
        for rows in (slice(0, MC), slice(MC, RIM + R)):
            for n in range(0, FS, NC):
                here = X[zc, rows, lanes_in]
                for sums, weight in ((gs, gfull), (vs, vfull)):
                    product = matmul(here, weight[half, :, n : n + NC])
                    if far:
                        product = (sums[zc, rows, n : n + NC] + product).astype(BF16).astype(F32)
                    sums[zc, rows, n : n + NC] = product

    def near_step(zc, _):
        products(zc, 0)
        return 0

    def far_step(zc, _):
        products(zc, 1)
        return 0

    gather_rest()
    mark("near_wait")
    for m in range(2):
        ready(m, True)
    mark("near")
    lax.fori_loop(0, 2, near_step, 0)
    mark("far_wait")
    for m in range(2):
        ready(m, False)
    pump("ffn")
    mark("far")
    lax.fori_loop(0, 2, far_step, 0)
    pump("conv0")
    mark("conv_f")

    def convolved(zc, _):
        RB = 64
        for r in range(0, R, RB):
            for n in range(0, FS, NC):
                lanes = slice(n, n + NC)
                gate = jnp.zeros((RB, NC), F32)
                value = jnp.zeros((RB, NC), F32)
                for j in range(KF):
                    start = RIM - (KF - 1) + j + r
                    gate = gate + gt[j : j + 1, lanes] * gs[zc, start : start + RB, lanes]
                    value = value + st[j : j + 1, lanes] * vs[zc, start : start + RB, lanes]
                hidden[zc, r : r + RB, lanes] = (silu(gate) * value).astype(BF16)

        return 0

    lax.fori_loop(0, 2, convolved, 0)
    mark("conv1")
    pump("conv1")

    HD = D // 4
    phase_ids = []

    def first_stage(p):
        mark(f"pump_down{p}")
        pump(f"down{p}")
        mark(f"ready2{p}")
        ready(2, p < 2, p % 2)
        half = (zh + p // 2) % 2
        i_o = [ids() for _ in range(4)]
        i_r = [ids() for _ in range(6)]
        phase_ids.append(i_r)
        order = ((zo, 1), (zl, 1), (zo, 0), (zl, 0))

        def down_rows(zi, ti, n, half=half, p=p):
            rows = pl.ds(pl.multiple_of(ti * SH, SH), SH)
            return matmul(hidden[zi, rows, :], dfull[half, p % 2, :, n : n + NCH])

        mark(f"down{p}")
        for k, (zi, far) in enumerate(order):
            ti = (t_c + 2 * far) % 4
            for n in range(0, HD, NCH):
                osend[p, k, :, n : n + NCH] = down_rows(zi, ti, n).astype(BF16)
            send(osend.at[p, k], cgot.at[p, k], i_o[k], P_c)
        mark(f"diag{p}")
        recv(cgot.at[p, 0], i_o[0])
        for n in range(0, HD, NCH):
            r2send[p, 2, :, n : n + NCH] = (
                down_rows(zo, t_x, n) + cgot[p, 0, :, n : n + NCH].astype(F32)
            ).astype(BF16)
        send(r2send.at[p, 2, pl.ds(0, HALF), :], r1got.at[p, pl.ds(0, HALF), :], i_r[0], P_x)
        send(r2send.at[p, 2, pl.ds(HALF, HALF), :], r1got.at[p, pl.ds(HALF, HALF), :], i_r[1], P_z)
        recv(cgot.at[p, 1], i_o[1])
        for n in range(0, HD, NCH):
            bx_sum[p % 2, :, n : n + NCH] = down_rows(zl, t_x, n) + cgot[p, 1, :, n : n + NCH].astype(F32)
        r2send[p, 0, 0:HALF, :] = bx_sum[p % 2, 0:HALF, :].astype(BF16)
        send(r2send.at[p, 0, pl.ds(0, HALF), :], r2got.at[p, 0, pl.ds(0, HALF), :], i_r[2], P_x)
        recv(cgot.at[p, 2], i_o[2])
        for n in range(0, HD, NCH):
            bz_sum[p % 2, :, n : n + NCH] = down_rows(zo, t, n) + cgot[p, 2, :, n : n + NCH].astype(F32)
        r2send[p, 1, HALF:, :] = bz_sum[p % 2, HALF:, :].astype(BF16)
        send(r2send.at[p, 1, pl.ds(HALF, HALF), :], r2got.at[p, 1, pl.ds(HALF, HALF), :], i_r[3], P_z)
        recv(cgot.at[p, 3], i_o[3])
        for n in range(0, HD, NCH):
            own_sum[:, p * HD + n : p * HD + n + NCH] = (
                down_rows(zl, t, n) + cgot[p, 3, :, n : n + NCH].astype(F32)
            )

    def second_stage(p):
        i_r = phase_ids[p]
        mark(f"r1wait{p}")
        first, second = pl.ds(0, HALF), pl.ds(HALF, HALF)
        recv(r1got.at[p, second, :], i_r[1])
        r2send[p, 0, HALF:, :] = (bx_sum[p % 2, HALF:, :] + r1got[p, HALF:, :].astype(F32)).astype(BF16)
        send(r2send.at[p, 0, second, :], r2got.at[p, 0, second, :], i_r[4], P_x)
        recv(r1got.at[p, first, :], i_r[0])
        r2send[p, 1, 0:HALF, :] = (bz_sum[p % 2, 0:HALF, :] + r1got[p, 0:HALF, :].astype(F32)).astype(BF16)
        send(r2send.at[p, 1, first, :], r2got.at[p, 1, first, :], i_r[5], P_z)

    first_stage(0)
    for p in range(1, 4):
        first_stage(p)
        second_stage(p - 1)
    second_stage(3)
    for p in range(4):
        i_r = phase_ids[p]
        half = (zh + p // 2) % 2
        mark(f"r2wait{p}")
        for h, (i_of_x, i_of_z) in enumerate(((i_r[2], i_r[5]), (i_r[4], i_r[3]))):
            recv(r2got.at[p, 0, pl.ds(h * HALF, HALF), :], i_of_x)
            recv(r2got.at[p, 1, pl.ds(h * HALF, HALF), :], i_of_z)
        mark(f"final{p}")
        for a in range(2):
            @pl.when(half == a)
            def _(a=a, p=p):
                for r in range(0, SH, RC):
                    here = slice(r, r + RC)
                    for j in range(HD // LANE):
                        from_ = slice(j * LANE, (j + 1) * LANE)
                        mine = slice(p * HD + j * LANE, p * HD + (j + 1) * LANE)
                        first = a * (D // 2) + j * KS + (p % 2) * LANE
                        cols = slice(first, first + LANE)
                        out[here, cols] = (
                            own_sum[here, mine]
                            + stream[here, cols].astype(F32)
                            + r2got[p, 0, here, from_].astype(F32)
                            + r2got[p, 1, here, from_].astype(F32)
                        ).astype(BF16)
    mark("drain")
    for f in pending:
        f()
    mark(None)
    assert counter[0] <= ssem.shape[0]
    assert len(moves) == NQ * (Z + 2)
    assert local_n[0] <= lsem.shape[0] - 4


def fused_dims(nsp, ntp, args):
    R, CH = args[0].shape
    NH = args[4].shape[1]
    D, F = args[12].shape[1], args[15].shape[1]
    fits = (
        nsp % 4 == 0 and nsp == 8 and ntp == 4
        and args[1].shape[1] == STATE and args[2].shape[1] == STATE
        and NH == 8 and CH == NH * HEAD and 2 * STATE == LANE
        and R % BLOCK == 0 and R % (ntp * 2 * RIM) == 0
        and D // nsp == 2 * LANE and D % 512 == 0 and F % LANE == 0
        and args[8].shape[0] <= 8 and args[17].shape[0] <= 8
    )
    FS = (F // LANE + 1) // 2 * LANE
    if not fits or FS % 256 or nsp % 8:
        return None
    return (R, CH, NH, D, F, FS, D // nsp, R // ntp)


def fused_on_device(nsp, ntp, dims, args):
    (
        xv, write, read, og, scores, extra, bias, rate, vtaps, wtaps, rtaps, ggain, wout, resid,
        fgain, gw, vw, gtaps, staps, dw,
    ) = args
    (R, CH, NH, D, F, FS, KS, SH) = dims
    Z, NB = nsp // 2, R // BLOCK
    rounds = max(1, (nsp - 2).bit_length())
    V = pltpu.VMEM
    msg_rows = STATE + 16
    scratch = [
        V((R, CH), BF16), V((CH, D), BF16),
        V((RIM, CH), BF16), V((2, STATE, LANE), BF16), V((8 + R, LANE), F32),
        V((R, LANE), BF16), V((NB, LANE, BLOCK), BF16), V((2 * NH, R), F32),
        V((NH, R), F32), V((R, NH), F32), V((NB, STATE, CH), F32), V((NB + 2, LANE), F32),
        V((msg_rows, CH), BF16), V((STATE + 8, CH), F32),
        V((rounds - 1, msg_rows, CH), BF16), V((rounds + 1, msg_rows, CH), BF16),
        V((R, CH), BF16), V((2, SH, D), BF16), V((2, SH, D), BF16),
        V((SH, D), BF16), V((SH, D), BF16), V((SH, D), F32), V((SH, D), BF16), V((SH, D), BF16),
        V((Z, KS, F), BF16), V((Z, KS, F), BF16), V((Z, F, KS), BF16),
        V((2, D // 2, FS), BF16), V((2, D // 2, FS), BF16), V((2, 2, FS, D // 4), BF16),
        V((2, RIM + R, D), BF16), V((2, RIM + R, FS), F32), V((2, RIM + R, FS), F32),
        V((2, R, FS), BF16), V((4, 4, SH, D // 4), BF16), V((4, 4, SH, D // 4), BF16),
        V((4, SH, D // 4), BF16), V((4, 3, SH, D // 4), BF16), V((4, 2, SH, D // 4), BF16),
        V((2, SH, D // 4), F32), V((2, SH, D // 4), F32),
        pltpu.SemaphoreType.DMA((288,)), pltpu.SemaphoreType.DMA((288,)),
        pltpu.SemaphoreType.DMA((80,)),
    ]
    vm, hbm = pl.BlockSpec(memory_space=pltpu.VMEM), pl.BlockSpec(memory_space=pl.ANY)
    return pl.pallas_call(
        functools.partial(fused_kernel, nsp, ntp, dims),
        out_shape=jax.ShapeDtypeStruct((SH, D), BF16),
        in_specs=[
            hbm, vm, vm, hbm, vm, vm, vm, vm, vm, vm, vm, vm, hbm, hbm, vm, hbm, hbm, vm, vm, hbm
        ],
        out_specs=vm,
        scratch_shapes=scratch,
        compiler_params=pltpu.CompilerParams(
            collective_id=0, has_side_effects=True, vmem_limit_bytes=67043328
        ),
    )(
        xv, write.T, read.T, og, scores.T, extra.T, bias.reshape(1, NH), rate.reshape(1, NH), vtaps,
        wtaps, rtaps, ggain.reshape(1, CH), wout, resid, fgain.reshape(1, D), gw, vw, gtaps, staps, dw,
    )


def on_device(nsp, ntp, *args):
    dims = fused_dims(nsp, ntp, args)
    if dims is None:
        return plain_on_device(*args)
    return fused_on_device(nsp, ntp, dims, args)


def solution(mesh):
    placed = (
        P("sp", "tp"),
        P("sp", "tp"),
        P("sp", "tp"),
        P("sp", "tp"),
        P("sp", "tp"),
        P("sp", "tp"),
        P("tp"),
        P("tp"),
        P(None, "tp"),
        P(None, "tp"),
        P(None, "tp"),
        P("tp"),
        P("tp", None),
        P("sp", None),
        P(),
        P("sp", "tp"),
        P("sp", "tp"),
        P(None, "tp"),
        P(None, "tp"),
        P("tp", "sp"),
    )
    return jax.shard_map(
        functools.partial(on_device, mesh.shape["sp"], mesh.shape["tp"]), mesh=mesh, in_specs=placed, out_specs=P(("sp", "tp"), None), check_vma=False
    )
```
